512 devices in a mesh: rep: 2 (over z_hi), fs: 32 (over z_lo, y), tp: 8 (over x, core).
Axes of the slice: x: 4, y: 8, z: 8 (z_hi: 2, z_lo: 4; z = z_hi * 4 + z_lo), core: 2. Of those that a mesh axis runs over, the one named last changes fastest.
Arguments:
- tokens: bfloat16 [32768, 2048], P(('rep', 'fs'), 'tp'), may hold values from -6 to 6
- mix_gain: float32 [2048], replicated, may hold values from 0.1 to 1.9
- query_w: bfloat16 [2048, 2048], P('fs', 'tp'), may hold values from -0.125 to 0.125
- key_w: bfloat16 [2048, 2048], P('fs', 'tp'), may hold values from -0.125 to 0.125
- value_w: bfloat16 [2048, 4096], P('fs', 'tp'), may hold values from -0.125 to 0.125
- head_gain: float32 [8, 512], replicated, may hold values from 0.1 to 1.9
- out_w: bfloat16 [4096, 2048], P('tp', 'fs'), may hold values from -0.09375 to 0.09375
- chan_gain: float32 [2048], replicated, may hold values from 0.1 to 1.9
- up_w: bfloat16 [2048, 4096], P('fs', 'tp'), may hold values from -0.125 to 0.125
- down_w: bfloat16 [4096, 2048], P('tp', 'fs'), may hold values from -0.09375 to 0.09375
Outputs:
- layer_out: bfloat16 [32768, 2048], P(('rep', 'fs'), 'tp')
The draws below stay inside these ranges and needn't reach their ends.
All inputs are finite; a program needn't handle non-finite values.
Results may differ from the reference program's by a relative error of at most 0.019.
Values may be sent and summed in bfloat16 or wider, within the bound.
A program may use at most 64 MiB of HBM per device.

```python
import jax
import jax.numpy as jnp
from jax import lax

D = 2048
HEADS = 8
DK = 256
DV = 512
FF = 4096
BLOCK = 128
TOK = 512
TOKENS = 32768
N_TP = 8


def block_scale(key, dims, shards, low, high):
    def one(dim, blocks):
        draws = jax.random.uniform(jax.random.fold_in(jax.random.fold_in(key, 6), dim), (blocks,), jnp.float32, low / len(shards), high / len(shards))
        return jnp.repeat(jnp.exp(draws), dims[dim] // blocks).reshape((-1,) + (1,) * (len(dims) - dim - 1))

    level = one(*shards[0])
    for cut in shards[1:]:
        level = level * one(*cut)
    return level


def noise(stream_key, shape, deviation, bound, shards=(), kind=jnp.bfloat16):
    values = jax.random.normal(stream_key, shape, jnp.float32) * deviation
    if len(shards) > 0:
        values = block_scale(stream_key, shape, shards, -0.22, 0.18) * values
    return jnp.clip(values, min=-bound, max=bound).astype(kind)


def setup_inputs(seed: int = 0) -> dict:
    splits = jax.random.split(jax.random.key(seed), 11)
    return {
        "tokens": noise(splits[0], (TOKENS, D), 1.0, 6.0, ((0, 64), (1, 8))),
        "mix_gain": jnp.clip(1.0 + 0.18 * jax.random.normal(splits[1], (D,), jnp.float32), 0.1, 1.9),
        "query_w": noise(splits[2], (D, D), D ** -0.5, 0.125, ((0, 32), (1, 8))),
        "key_w": noise(splits[3], (D, D), D ** -0.5, 0.125, ((0, 32), (1, 8))),
        "value_w": noise(splits[4], (D, HEADS * DV), D ** -0.5, 0.125, ((0, 32), (1, 8))),
        "head_gain": jnp.clip(1.0 + 0.18 * jax.random.normal(splits[5], (HEADS, DV), jnp.float32), 0.1, 1.9),
        "out_w": noise(splits[6], (HEADS * DV, D), (HEADS * DV) ** -0.5, 0.09375, ((0, 8), (1, 32))),
        "chan_gain": jnp.clip(1.0 + 0.18 * jax.random.normal(splits[7], (D,), jnp.float32), 0.1, 1.9),
        "up_w": noise(splits[8], (D, FF), D ** -0.5, 0.125, ((0, 32), (1, 8))),
        "down_w": noise(splits[9], (FF, D), FF ** -0.5, 0.09375, ((0, 8), (1, 32))),
    }


EPS = 1e-06
HEAD_EPS = 0.05
THETA = 10000.0

def norm_rows(rows, gain):
    values = rows.astype(jnp.float32)
    scale = lax.rsqrt(lax.optimization_barrier(jnp.mean(values * values, axis=-1, keepdims=True)) + EPS)
    return (values * scale * gain).astype(jnp.bfloat16)

def rotate(field, places):
    half = field.shape[-1] // 2
    inverse = THETA ** (-jnp.arange(half, dtype=jnp.float32) / half)
    angles = places[:, None] * inverse
    cosine = jnp.cos(angles)[:, None, :]
    sine = jnp.sin(angles)[:, None, :]
    first = field[..., :half]
    second = field[..., half:]
    return jnp.concatenate([first * cosine - second * sine, second * cosine + first * sine], axis=-1)

def retain(query, keys, values, log_rate):
    count = query.shape[0] // BLOCK
    q_blocks = query.reshape(count, BLOCK, query.shape[1])
    k_blocks = keys.reshape(count, BLOCK, keys.shape[1])
    v_blocks = values.reshape(count, BLOCK, values.shape[1])
    place = jnp.arange(BLOCK, dtype=jnp.float32)
    offset = place[:, None] - place[None, :]
    mask = jnp.where(offset >= 0, jnp.exp(log_rate * jnp.maximum(offset, 0.0)), 0.0)
    q_decay = jnp.exp(log_rate * (place + 1.0))
    k_decay = jnp.exp(log_rate * (BLOCK - 1.0 - place))
    block_decay = jnp.exp(log_rate * BLOCK)

    def advance(state, item):
        q_part, k_part, v_part = item
        scores = jnp.dot(q_part, k_part.T, preferred_element_type=jnp.float32)
        weights = (scores * mask).astype(jnp.bfloat16)
        result = jnp.dot(weights, v_part, preferred_element_type=jnp.float32)
        q_scaled = (q_part.astype(jnp.float32) * q_decay[:, None]).astype(jnp.bfloat16)
        result = result + jnp.dot(q_scaled, state.astype(jnp.bfloat16), preferred_element_type=jnp.float32)
        k_scaled = (k_part.astype(jnp.float32) * k_decay[:, None]).astype(jnp.bfloat16)
        state = state * block_decay + jnp.dot(k_scaled.T, v_part, preferred_element_type=jnp.float32)
        return (state, result)
    start = jnp.zeros((query.shape[1], values.shape[1]), jnp.float32)
    _, outputs = lax.scan(advance, start, (q_blocks, k_blocks, v_blocks))
    return outputs.reshape(count * BLOCK, values.shape[1])

def grouped_sum(left, right):
    width = left.shape[1] // N_TP
    total = jnp.zeros((left.shape[0], right.shape[1]), jnp.float32)
    for group in range(N_TP):
        term = jnp.dot(left[:, group * width:(group + 1) * width], right[group * width:(group + 1) * width], preferred_element_type=jnp.float32).astype(jnp.bfloat16)
        term = lax.optimization_barrier(term)
        total = total + term.astype(jnp.float32)
    return total

def reference(tokens, mix_gain, query_w, key_w, value_w, head_gain, out_w, chan_gain, up_w, down_w):
    normed = norm_rows(tokens, mix_gain)
    qraw = jnp.dot(normed, query_w, preferred_element_type=jnp.float32)
    kraw = jnp.dot(normed, key_w, preferred_element_type=jnp.float32)
    vraw = jnp.dot(normed, value_w, preferred_element_type=jnp.float32)
    places = (jnp.arange(TOKENS, dtype=jnp.int32) % TOK).astype(jnp.float32)
    query = rotate(qraw.reshape(TOKENS, HEADS, DK), places).astype(jnp.bfloat16)
    keys = (rotate(kraw.reshape(TOKENS, HEADS, DK), places) * DK ** (-0.5)).astype(jnp.bfloat16)
    values = vraw.reshape(TOKENS, HEADS, DV).astype(jnp.bfloat16)
    heads = jnp.arange(HEADS, dtype=jnp.int32).astype(jnp.float32)
    log_rate = jnp.log1p(-jnp.exp2(-5.0 - heads))
    count = TOKENS // TOK
    per_head = jax.vmap(retain, in_axes=(1, 1, 1, 0), out_axes=1)

    def one_sequence(item):
        return per_head(item[0], item[1], item[2], log_rate)
    retained = lax.map(one_sequence, (query.reshape(count, TOK, HEADS, DK), keys.reshape(count, TOK, HEADS, DK), values.reshape(count, TOK, HEADS, DV)))
    retained = retained.reshape(TOKENS, HEADS, DV)
    scale = lax.rsqrt(lax.optimization_barrier(jnp.mean(retained * retained, axis=-1, keepdims=True)) + HEAD_EPS)
    head_out = (retained * scale * head_gain).astype(jnp.bfloat16).reshape(TOKENS, HEADS * DV)
    middle = (tokens.astype(jnp.float32) + grouped_sum(head_out, out_w)).astype(jnp.bfloat16)
    chan_normed = norm_rows(middle, chan_gain)
    upward = jnp.dot(chan_normed, up_w, preferred_element_type=jnp.float32)
    hidden = jnp.square(jax.nn.relu(upward)).astype(jnp.bfloat16)
    return (middle.astype(jnp.float32) + grouped_sum(hidden, down_w)).astype(jnp.bfloat16)
```

```python
import functools
import heapq

import jax
import jax.numpy as jnp
from jax import lax
from jax.experimental import pallas as pl
from jax.experimental.pallas import tpu as pltpu
from jax.sharding import PartitionSpec as P

DK = 256
DV = 512
BLOCK = 128


EPS = 1e-06
HEAD_EPS = 0.05
THETA = 10000.0


def neighbours(route, a, b, unit):
    out = []
    two = lambda k: 1 if k % 2 == 0 else -1
    if route == "A":
        fw = 4 if unit % 4 < 2 else 3
        bw = 7 - fw
        if b == 0:
            if 0 <= a < fw: out.append(("y", 1))
            if 0 >= a > -bw: out.append(("y", -1))
            out += [("z", 1), ("z", -1)]
        elif abs(b) == 1 and two(a) == b:
            out.append(("z", b))
    else:
        fw = 4 if b % 2 == 0 else 3
        bw = 7 - fw
        if a == 0:
            if b == 0: out += [("z", 1), ("z", -1)]
            elif abs(b) == 1 and two(unit // 2) == b: out.append(("z", b))
        if 0 <= a < fw: out.append(("y", 1))
        if 0 >= a > -bw: out.append(("y", -1))
    return out

def simulate(routes, group, service=1.45, latency=1.8, lead=3.2, start=None):
    start = start or [0.0] * len(routes)
    def down(u, a, b):
        n = neighbours(routes[u], a, b, u)
        return max([0] + [1 + down(u, a + (s if ax == "y" else 0), b + (s if ax == "z" else 0)) for ax, s in n])
    free = {(ax, s): 0.0 for ax in "yz" for s in (1, -1)}
    pending = {k: [] for k in free}
    events = []
    actions = []
    seq = 0
    arrivals = [(start[u], 0, u, 0, 0) for u in range(len(routes))]
    heapq.heapify(arrivals)
    index = {}
    counts = [0] * len(routes)
    now = 0.0
    arrived = {}
    while arrivals or any(pending.values()):
        t_link = min([max(free[k], min(p[2] for p in pending[k])) for k in free if pending[k]], default=float("inf"))
        t_arr = arrivals[0][0] if arrivals else float("inf")
        if t_arr <= t_link:
            t, hop, u, a, b = heapq.heappop(arrivals)
            arrived[(u, a, b)] = t
            if (a, b) != (0, 0):
                index[(u, a, b)] = counts[u]; counts[u] += 1
                actions.append((t, 0, ("wait", u, a, b)))
            for ax, s in neighbours(routes[u], a, b, u):
                na, nb = a + (s if ax == "y" else 0), b + (s if ax == "z" else 0)
                pending[(ax, s)].append((group[u], -(1 + down(u, na, nb)), t, u, a, b, na, nb))
        else:
            k = min((k for k in free if pending[k]), key=lambda k: max(free[k], min(p[2] for p in pending[k])))
            t0 = t_link
            ready = [p for p in pending[k] if p[2] <= t0 + 1e-9]
            p = min(ready)
            pending[k].remove(p)
            free[k] = t0 + service
            g, d, t, u, a, b, na, nb = p
            actions.append((max(t, t0 - lead), 1, ("send", u, a, b, na, nb, k)))
            heapq.heappush(arrivals, (t0 + service + latency, 1, u, na, nb))
    actions.sort(key=lambda x: (x[0], x[1]))
    return actions, index, counts, arrived


ROUTES = "ABABA"
GROUPS = (0, 0, 1, 2, 2)
NY, NZ = 8, 4
MESH = pl.DeviceIdType.MESH


def gather_kernel(*refs):
    parts, units = refs[:5], refs[5:10]
    local_sem, send_sem, recv_sem = refs[10:]
    rep, fs = lax.axis_index("rep"), lax.axis_index("fs")
    z, y = fs // NY, fs % NY
    z_up, z_down = (z + 1) % NZ, (z + NZ - 1) % NZ
    away = {
        ("y", 1): (rep, z * NY + (y + 1) % NY),
        ("y", -1): (rep, z * NY + (y + NY - 1) % NY),
        ("z", 1): ((rep + (z + 1) // NZ) % 2, z_up * NY + y),
        ("z", -1): ((rep + (NZ - z) // NZ) % 2, z_down * NY + y),
    }
    target = {k: {"rep": r, "fs": f} for k, (r, f) in away.items()}

    def slot(a, b):
        at = ((z - b + NZ) % NZ) * NY + (y - a + NY) % NY
        return pl.ds(pl.multiple_of(at * 64, 64), 64)

    barrier = pltpu.get_barrier_semaphore()
    for k in target:
        pl.semaphore_signal(barrier, inc=1, device_id=target[k], device_id_type=MESH)
    local = []
    for u in range(5):
        copy = pltpu.make_async_copy(parts[u], units[u].at[slot(0, 0)], local_sem.at[u])
        copy.start()
        local.append(copy)
    for copy in local:
        copy.wait()
    pl.semaphore_wait(barrier, 4)

    actions, index, counts, _ = simulate(ROUTES, GROUPS)

    def copy_of(n, u, a, b, na, nb, k):
        return pltpu.make_async_remote_copy(
            src_ref=units[u].at[slot(a, b)],
            dst_ref=units[u].at[slot(a, b)],
            send_sem=send_sem.at[n],
            recv_sem=recv_sem.at[u, index[u, na, nb]],
            device_id=target[k],
            device_id_type=MESH,
        )

    sends = []
    for _, _, action in actions:
        if action[0] == "wait":
            _, u, a, b = action
            here = units[u].at[slot(a, b)]
            pltpu.make_async_copy(here, here, recv_sem.at[u, index[u, a, b]]).wait()
        else:
            copy = copy_of(len(sends), *action[1:])
            copy.start()
            sends.append(copy)
    for copy in sends:
        copy.wait_send()


def gather_units(parts):
    return pl.pallas_call(
        gather_kernel,
        out_shape=[jax.ShapeDtypeStruct((2048, 512), jnp.bfloat16)] * 5,
        in_specs=[pl.BlockSpec(memory_space=pl.ANY)] * 5,
        out_specs=[pl.BlockSpec(memory_space=pltpu.VMEM)] * 5,
        scratch_shapes=[
            pltpu.SemaphoreType.DMA((5,)),
            pltpu.SemaphoreType.DMA((155,)),
            pltpu.SemaphoreType.DMA((5, 31)),
        ],
        compiler_params=pltpu.CompilerParams(
            collective_id=0, has_side_effects=True, vmem_limit_bytes=60 << 20
        ),
        name="gather_units",
    )(*parts)


def in_order(blocks, dim):
    shape = list(blocks.shape[1:])
    shape[dim] *= blocks.shape[0]
    return jnp.moveaxis(blocks, 0, dim).reshape(shape)


def copy_for_each(value, axis):
    count = lax.axis_size(axis)
    return lax.all_to_all(
        jnp.broadcast_to(value[None], (count, *value.shape)), axis, 0, 0, tiled=True
    )


def gathered_copies(value, axis, dim):
    return in_order(copy_for_each(value, axis), dim)


def cut_along(value, dim, count):
    shape = value.shape
    blocks = value.reshape(*shape[:dim], count, shape[dim] // count, *shape[dim + 1 :])
    return jnp.moveaxis(blocks, dim, 0)


def sum_at_owner(value, axis, dim):
    count = lax.axis_size(axis)
    blocks = lax.all_to_all(cut_along(value, dim, count), axis, 0, 0, tiled=True)
    return jnp.sum(blocks.astype(jnp.float32), axis=0)


def norm_rows(rows, gain):
    values = rows.astype(jnp.float32)
    scale = lax.rsqrt(jnp.mean(values * values, axis=-1, keepdims=True) + EPS)
    return (values * scale * gain).astype(jnp.bfloat16)


def rotate(field, places):
    half = field.shape[-1] // 2
    inverse = THETA ** (-jnp.arange(half, dtype=jnp.float32) / half)
    angles = places[:, None] * inverse
    cosine = jnp.cos(angles)[:, None, :]
    sine = jnp.sin(angles)[:, None, :]
    first = field[..., :half]
    second = field[..., half:]
    return jnp.concatenate(
        [first * cosine - second * sine, second * cosine + first * sine], axis=-1
    )


def retain(query, keys, values, log_rate):
    count = query.shape[0] // BLOCK
    q_blocks = query.reshape(count, BLOCK, query.shape[1])
    k_blocks = keys.reshape(count, BLOCK, keys.shape[1])
    v_blocks = values.reshape(count, BLOCK, values.shape[1])
    place = jnp.arange(BLOCK, dtype=jnp.float32)
    offset = place[:, None] - place[None, :]
    mask = jnp.where(offset >= 0, jnp.exp(log_rate * jnp.maximum(offset, 0.0)), 0.0)
    q_decay = jnp.exp(log_rate * (place + 1.0))
    k_decay = jnp.exp(log_rate * (BLOCK - 1.0 - place))
    block_decay = jnp.exp(log_rate * BLOCK)

    def advance(state, item):
        q_part, k_part, v_part = item
        scores = jnp.dot(q_part, k_part.T, preferred_element_type=jnp.float32)
        weights = (scores * mask).astype(jnp.bfloat16)
        result = jnp.dot(weights, v_part, preferred_element_type=jnp.float32)
        q_scaled = (q_part.astype(jnp.float32) * q_decay[:, None]).astype(jnp.bfloat16)
        result = result + jnp.dot(
            q_scaled, state.astype(jnp.bfloat16), preferred_element_type=jnp.float32
        )
        k_scaled = (k_part.astype(jnp.float32) * k_decay[:, None]).astype(jnp.bfloat16)
        state = state * block_decay + jnp.dot(
            k_scaled.T, v_part, preferred_element_type=jnp.float32
        )
        return (state, result)

    start = jnp.zeros((query.shape[1], values.shape[1]), jnp.float32)
    _, outputs = lax.scan(advance, start, (q_blocks, k_blocks, v_blocks))
    return outputs.reshape(count * BLOCK, values.shape[1])


def shards(tokens, mix_gain, query_w, key_w, value_w, head_gain, out_w, chan_gain, up_w, down_w):
    rows = tokens.shape[0]
    local = query_w.shape[1] // DK
    parts = (jnp.concatenate([query_w, key_w], axis=1), value_w, out_w.T, up_w, down_w.T)
    both, value_all, out_turned, up_all, down_turned = gather_units(parts)
    query_all, key_all = both[:, :DK], both[:, DK:]
    out_all, down_all = out_turned.T, down_turned.T
    whole = gathered_copies(tokens, "tp", 1)
    normed = norm_rows(whole, mix_gain)
    qraw = jnp.dot(normed, query_all, preferred_element_type=jnp.float32)
    kraw = jnp.dot(normed, key_all, preferred_element_type=jnp.float32)
    vraw = jnp.dot(normed, value_all, preferred_element_type=jnp.float32)
    places = jnp.arange(rows, dtype=jnp.int32).astype(jnp.float32)
    query = rotate(qraw.reshape(rows, local, DK), places).astype(jnp.bfloat16)
    keys = (rotate(kraw.reshape(rows, local, DK), places) * DK ** (-0.5)).astype(jnp.bfloat16)
    values = vraw.reshape(rows, local, DV).astype(jnp.bfloat16)
    first_head = lax.axis_index("tp") * local
    heads = (first_head + jnp.arange(local, dtype=jnp.int32)).astype(jnp.float32)
    log_rate = jnp.log1p(-jnp.exp2(-5.0 - heads))
    retained = jax.vmap(retain, in_axes=(1, 1, 1, 0), out_axes=1)(query, keys, values, log_rate)
    gains = lax.dynamic_slice_in_dim(head_gain, first_head, local, 0)
    scale = lax.rsqrt(jnp.mean(retained * retained, axis=-1, keepdims=True) + HEAD_EPS)
    head_out = (retained * scale * gains).astype(jnp.bfloat16).reshape(rows, local * DV)
    mixer_terms = jnp.dot(head_out, out_all, preferred_element_type=jnp.float32)
    mixed = sum_at_owner(mixer_terms.astype(jnp.bfloat16), "tp", 1)
    middle = (tokens.astype(jnp.float32) + mixed).astype(jnp.bfloat16)
    whole_middle = gathered_copies(middle, "tp", 1)
    chan_normed = norm_rows(whole_middle, chan_gain)
    upward = jnp.dot(chan_normed, up_all, preferred_element_type=jnp.float32)
    hidden = jnp.square(jax.nn.relu(upward)).astype(jnp.bfloat16)
    chan_terms = jnp.dot(hidden, down_all, preferred_element_type=jnp.float32)
    channel = sum_at_owner(chan_terms.astype(jnp.bfloat16), "tp", 1)
    return (middle.astype(jnp.float32) + channel).astype(jnp.bfloat16)


def solution(mesh):
    placed = (
        P(("rep", "fs"), "tp"),
        P(),
        P("fs", "tp"),
        P("fs", "tp"),
        P("fs", "tp"),
        P(),
        P("tp", "fs"),
        P(),
        P("fs", "tp"),
        P("tp", "fs"),
    )
    return jax.shard_map(
        shards, mesh=mesh, in_specs=placed, out_specs=P(("rep", "fs"), "tp"), check_vma=False
    )
```

```python
import heapq

import jax
import jax.numpy as jnp
import numpy as np
from jax import lax
from jax.experimental import pallas as pl
from jax.experimental.pallas import tpu as pltpu
from jax.sharding import PartitionSpec as P

ROWS = 512
D = 2048
DK = 256
DV = 512
EPS = 1e-06
HEAD_EPS = 0.05
THETA = 10000.0
NX, NY, NZ = 4, 8, 4
ROUTES = "ABABA"
GROUPS = (0, 0, 1, 2, 2)
STARTS = (0.0, 0.0, 3.0, 3.0, 3.0)
MESH = pl.DeviceIdType.MESH
BF, F32 = jnp.bfloat16, jnp.float32


def neighbours(route, a, b, unit):
    out = []
    two = lambda k: 1 if k % 2 == 0 else -1
    if route == "A":
        fw = 4 if unit % 4 < 2 else 3
        bw = 7 - fw
        if b == 0:
            if 0 <= a < fw: out.append(("y", 1))
            if 0 >= a > -bw: out.append(("y", -1))
            out += [("z", 1), ("z", -1)]
        elif abs(b) == 1 and two(a) == b:
            out.append(("z", b))
    else:
        fw = 4 if b % 2 == 0 else 3
        bw = 7 - fw
        if a == 0:
            if b == 0: out += [("z", 1), ("z", -1)]
            elif abs(b) == 1 and two(unit // 2) == b: out.append(("z", b))
        if 0 <= a < fw: out.append(("y", 1))
        if 0 >= a > -bw: out.append(("y", -1))
    return out

def simulate(routes, group, service=1.45, latency=1.8, lead=3.2, start=None):
    start = start or [0.0] * len(routes)
    def down(u, a, b):
        n = neighbours(routes[u], a, b, u)
        return max([0] + [1 + down(u, a + (s if ax == "y" else 0), b + (s if ax == "z" else 0)) for ax, s in n])
    free = {(ax, s): 0.0 for ax in "yz" for s in (1, -1)}
    pending = {k: [] for k in free}
    events = []
    actions = []
    seq = 0
    arrivals = [(start[u], 0, u, 0, 0) for u in range(len(routes))]
    heapq.heapify(arrivals)
    index = {}
    counts = [0] * len(routes)
    now = 0.0
    arrived = {}
    while arrivals or any(pending.values()):
        t_link = min([max(free[k], min(p[2] for p in pending[k])) for k in free if pending[k]], default=float("inf"))
        t_arr = arrivals[0][0] if arrivals else float("inf")
        if t_arr <= t_link:
            t, hop, u, a, b = heapq.heappop(arrivals)
            arrived[(u, a, b)] = t
            if (a, b) != (0, 0):
                index[(u, a, b)] = counts[u]; counts[u] += 1
                actions.append((t, 0, ("wait", u, a, b)))
            for ax, s in neighbours(routes[u], a, b, u):
                na, nb = a + (s if ax == "y" else 0), b + (s if ax == "z" else 0)
                pending[(ax, s)].append((group[u], -(1 + down(u, na, nb)), t, u, a, b, na, nb))
        else:
            k = min((k for k in free if pending[k]), key=lambda k: max(free[k], min(p[2] for p in pending[k])))
            t0 = t_link
            ready = [p for p in pending[k] if p[2] <= t0 + 1e-9]
            p = min(ready)
            pending[k].remove(p)
            free[k] = t0 + service
            g, d, t, u, a, b, na, nb = p
            actions.append((max(t, t0 - lead), 1, ("send", u, a, b, na, nb, k)))
            heapq.heappush(arrivals, (t0 + service + latency, 1, u, na, nb))
    actions.sort(key=lambda x: (x[0], x[1]))
    return actions, index, counts, arrived


def turned_dot(left, right):
    return lax.dot_general(left, right, (((1,), (1,)), ((), ())), preferred_element_type=F32)


def layer_kernel(
    tokens, mix_gain, query_w, key_w, value_w, head_gain, out_w, chan_gain, up_w, down_w, cosine, sine,
    result,
    w_both, w_value, w_out, w_up, w_down,
    blocks, normed, middle, turn_in, mix_row, chan_row, head_rows, cos_tab, sin_tab, decay,
    raw, query, keys, values, head_out, hidden,
    give1, take1, own1, move1, plain1, left1, right1, pass1,
    give2, take2, own2, move2, left2, right2, pass2,
    local_sem, send_sem, recv_sem,
):
    rep, fs, tp = lax.axis_index("rep"), lax.axis_index("fs"), lax.axis_index("tp")
    z, y = fs // NY, fs % NY
    x, core = tp // 2, tp % 2
    units = (w_both, w_value, w_out, w_up, w_down)
    target = {
        ("y", 1): {"fs": z * NY + (y + 1) % NY},
        ("y", -1): {"fs": z * NY + (y + NY - 1) % NY},
        ("z", 1): {"rep": (rep + (z + 1) // NZ) % 2, "fs": ((z + 1) % NZ) * NY + y},
        ("z", -1): {"rep": (rep + (NZ - z) // NZ) % 2, "fs": ((z + NZ - 1) % NZ) * NY + y},
        "right": {"tp": ((x + 1) % NX) * 2 + core},
        "left": {"tp": ((x + NX - 1) % NX) * 2 + core},
        "partner": {"tp": x * 2 + (1 - core)},
    }
    barrier = pltpu.get_barrier_semaphore()
    for k in target:
        pl.semaphore_signal(barrier, inc=1, device_id=target[k], device_id_type=MESH)

    def slot(a, b):
        at = ((z - b + NZ) % NZ) * NY + (y - a + NY) % NY
        return pl.ds(pl.multiple_of(at * 64, 64), 64)

    mine = slot(0, 0)
    local = []

    def bring(source, dest):
        copy = pltpu.make_async_copy(source, dest, local_sem.at[len(local)])
        copy.start()
        local.append(copy)

    bring(tokens, blocks.at[tp])
    bring(query_w, w_both.at[mine, 0:DK])
    bring(key_w, w_both.at[mine, DK : 2 * DK])
    bring(value_w, w_value.at[mine])
    bring(out_w, turn_in.at[0])
    bring(down_w, turn_in.at[1])
    bring(up_w, w_up.at[mine])
    bring(mix_gain, mix_row)
    bring(chan_gain, chan_row)
    bring(head_gain, head_rows)
    bring(cosine, cos_tab)
    bring(sine, sin_tab)
    for copy in local[:4]:
        copy.wait()
    pl.semaphore_wait(barrier, len(target))

    sends, names = [], {}

    def number(name):
        return names.setdefault(name, len(names))

    def send(source, dest, to, name):
        copy = pltpu.make_async_remote_copy(
            src_ref=source,
            dst_ref=dest,
            send_sem=send_sem.at[len(sends)],
            recv_sem=recv_sem.at[number(name)],
            device_id=target[to],
            device_id_type=MESH,
        )
        copy.start()
        sends.append(copy)

    def arrive(dest, name):
        pltpu.make_async_copy(dest, dest, recv_sem.at[number(name)]).wait()

    actions = simulate(ROUTES, GROUPS, start=STARTS)[0]
    position = [0]
    turned = []

    def turn():
        for copy in local[4:]:
            copy.wait()
        w_out[mine, :] = turn_in[0].T
        w_down[mine, :] = turn_in[1].T

    def step_weights():
        _, _, action = actions[position[0]]
        position[0] += 1
        if action[0] == "wait":
            _, u, a, b = action
            arrive(units[u].at[slot(a, b)], ("w", u, a, b))
        else:
            _, u, a, b, na, nb, k = action
            send(units[u].at[slot(a, b)], units[u].at[slot(a, b)], k, ("w", u, na, nb))

    def at(time):
        while position[0] < len(actions) and actions[position[0]][0] <= time:
            step_weights()

    def need(u, planes=(0, 1, -1, 2, -2)):
        last = max(i for i, c in enumerate(actions) if c[2][0] == "wait" and c[2][1] == u and c[2][3] in planes)
        while position[0] <= last:
            step_weights()

    def block_of(o, c):
        return ((x + o + NX) % NX) * 2 + c

    def gather(view, tag, times, arrived=None):
        def to(o, h, k, name):
            send(view(o, core, h), view(o, core, h), k, (tag, *name))

        to(0, 0, "right", (-1, 0))
        to(0, 1, "left", (1, 1))
        to(0, 1, "right", (-1, 1))
        to(0, 0, "left", (1, 0))
        to(0, 0, "partner", ("p", 0, 0))
        to(0, 1, "partner", ("p", 0, 1))
        order = [(-1, 0), (1, 1), (-1, 1), (1, 0), (-2, 0), (2, 1)]
        for (o, h), time in zip(order, times):
            at(time)
            arrive(view(o, core, h), (tag, o, h))
            if (o, h) == (-1, 0):
                to(o, h, "right", (-2, 0))
            if (o, h) == (1, 1):
                to(o, h, "left", (2, 1))
            to(o, h, "partner", ("p", o, h))
            if arrived and (o, h) in ((-1, 1), (1, 0), (2, 1)):
                arrived(o, core)
        for o, h in [(0, 0), (0, 1)] + order:
            arrive(view(o, 1 - core, h), (tag, "p", o, h))
            if arrived and (o, h) in ((0, 1), (-1, 1), (1, 0), (2, 1)):
                arrived(o, 1 - core)

    def token_view(o, c, h):
        return blocks.at[block_of(o, c), pl.ds(h * 256, 256)]

    at(0.0)
    rate = jnp.float32(0.0)
    for h in range(8):
        rate = jnp.where(tp == h, jnp.float32(np.log1p(-(2.0 ** (-5 - h)))), rate)
    gather_times = (5.0, 5.2, 7.8, 8.0, 10.6, 10.8)

    started = [False]

    def begin():
        turn()
        offset = (
            lax.broadcasted_iota(jnp.int32, (128, 128), 0) - lax.broadcasted_iota(jnp.int32, (128, 128), 1)
        ).astype(F32)
        for n in range(4):
            value = jnp.exp(rate * jnp.maximum(offset + 128.0 * n, 0.0))
            decay[n] = jnp.where(offset + 128.0 * n >= 0, value, 0.0)

    begin()
    gather(token_view, "t", gather_times)

    at(12.0)

    @pl.loop(0, ROWS // 64)
    def _(i):
        rows = pl.ds(pl.multiple_of(i * 64, 64), 64)
        total = jnp.zeros((64, 256), F32)
        for b in range(8):
            part = blocks[b, rows, :].astype(F32)
            total = total + part * part
        scale = lax.rsqrt(jnp.sum(total, axis=-1, keepdims=True) * (1.0 / D) + EPS)
        for b in range(8):
            columns = slice(b * 256, (b + 1) * 256)
            normed[rows, columns] = (blocks[b, rows, :].astype(F32) * scale * mix_row[:, columns]).astype(BF)

    def project(weights, tile, store):
        @pl.loop(0, 512 // tile)
        def _(i):
            columns = pl.ds(pl.multiple_of(i * tile, tile), tile)
            store(columns, jnp.dot(normed[...], weights[:, columns], preferred_element_type=F32))

    def keep_raw(columns, value):
        raw[:, columns] = value

    def keep_values(columns, value):
        values[:, columns] = value.astype(BF)

    def keep_hidden(columns, value):
        value = jnp.maximum(value, 0.0)
        hidden[:, columns] = (value * value).astype(BF)

    need(0)
    project(w_both, 256, keep_raw)
    need(1)
    at(31.0)
    project(w_value, 256, keep_values)

    @pl.loop(0, ROWS // 64)
    def _(i):
        rows = pl.ds(pl.multiple_of(i * 64, 64), 64)
        c, s = cos_tab[rows, :], sin_tab[rows, :]
        for start, dest, factor in ((0, query, 1.0), (DK, keys, DK**-0.5)):
            first, second = raw[rows, start : start + 128], raw[rows, start + 128 : start + 256]
            dest[rows, 0:128] = ((first * c - second * s) * factor).astype(BF)
            dest[rows, 128:256] = ((second * c + first * s) * factor).astype(BF)

    at(33.0)
    gain = head_rows[pl.ds(tp, 1), :]
    for i in range(4):
        rows = slice(i * 128, (i + 1) * 128)
        total = jnp.zeros((128, DV), F32)
        for j in range(i + 1):
            there = slice(j * 128, (j + 1) * 128)
            score = turned_dot(query[rows, :], keys[there, :]) * decay[i - j]
            total = total + jnp.dot(score.astype(BF), values[there, :], preferred_element_type=F32)
        scale = lax.rsqrt(jnp.mean(total * total, axis=-1, keepdims=True) + HEAD_EPS)
        part = (total * scale * gain).astype(BF)
        head_out[i, 0] = part[0:64]
        head_out[i, 1] = part[64:128]
        at(33.0 + 0.4 * (i + 1))

    planes = (0, 1, -1, 2)
    reached = {0: (0,), 1: (1,), -1: (-1,), 2: (2, -2)}

    def plane(b):
        return (z - b + NZ) % NZ

    def offset_rows(o, h):
        return pl.ds(pl.multiple_of(((x + o + NX) % NX) * 64 + h * 32, 32), 32)

    def exchange(n, b):
        weights = w_out[pl.ds(pl.multiple_of(plane(b) * 512, 512), 512), :]
        give1[n] = turned_dot(head_out[:, 1 - core].reshape(256, 512), weights).astype(BF)
        own1[n] = turned_dot(head_out[:, core].reshape(256, 512), weights)
        send(give1.at[n], take1.at[n], "partner", ("m", n))

    def part(n, o, h):
        rows = offset_rows(o, h)
        return own1[n, rows, :] + take1[n, rows, :].astype(F32)

    half = (slice(0, 32), slice(32, 64))

    def spread(n):
        arrive(take1.at[n], ("m", n))
        move1[n, 0] = part(n, 2, 0).astype(BF)
        move1[n, 1] = part(n, 2, 1).astype(BF)
        plain1[n, 0] = part(n, 1, 1).astype(BF)
        plain1[n, 1] = part(n, -1, 0).astype(BF)
        send(move1.at[n, 0], pass1.at[n, 0], "right", ("m2", n, 0))
        send(move1.at[n, 1], pass1.at[n, 1], "left", ("m2", n, 1))
        send(plain1.at[n, 0], left1.at[n, half[1]], "right", ("m1", n, 0))
        send(plain1.at[n, 1], right1.at[n, half[0]], "left", ("m1", n, 1))

    def merge(n):
        arrive(pass1.at[n, 0], ("m2", n, 0))
        move1[n, 2] = (part(n, 1, 0) + pass1[n, 0].astype(F32)).astype(BF)
        arrive(pass1.at[n, 1], ("m2", n, 1))
        move1[n, 3] = (part(n, -1, 1) + pass1[n, 1].astype(F32)).astype(BF)
        send(move1.at[n, 2], left1.at[n, half[0]], "right", ("m3", n, 0))
        send(move1.at[n, 3], right1.at[n, half[1]], "left", ("m3", n, 1))

    my_rows = pl.ds(pl.multiple_of(tp * 64, 64), 64)

    def settle(n, b):
        arrive(left1.at[n, half[1]], ("m1", n, 0))
        arrive(right1.at[n, half[0]], ("m1", n, 1))
        arrive(left1.at[n, half[0]], ("m3", n, 0))
        arrive(right1.at[n, half[1]], ("m3", n, 1))
        rows = pl.ds(pl.multiple_of(x * 64, 64), 64)
        total = own1[n, rows, :] + take1[n, rows, :].astype(F32)
        total = total + left1[n].astype(F32) + right1[n].astype(F32)
        for j in range(2):
            here = total[:, j * 256 : (j + 1) * 256] + blocks[2 * plane(b) + j, my_rows, :].astype(F32)
            columns = pl.ds(pl.multiple_of(plane(b) * 512 + j * 256, 256), 256)
            middle[my_rows, columns] = here.astype(BF)

    for n, b in enumerate(planes):
        need(2, reached[b])
        exchange(n, b)
        if n >= 1:
            spread(n - 1)
        if n >= 2:
            merge(n - 2)
    base = 46.0
    at(base + 1.0)
    spread(3)
    at(base + 2.0)
    merge(2)
    at(base + 4.0)
    merge(3)
    for n, b in enumerate(planes):
        at(base + 4.0 + n)
        settle(n, b)

    def middle_view(o, c, h):
        return middle.at[pl.ds(pl.multiple_of(block_of(o, c) * 64 + h * 32, 32), 32)]

    def norm_block(o, c):
        rows = pl.ds(pl.multiple_of(block_of(o, c) * 64, 64), 64)
        total = jnp.zeros((64, 256), F32)
        for b in range(8):
            chunk = middle[rows, b * 256 : (b + 1) * 256].astype(F32)
            total = total + chunk * chunk
        scale = lax.rsqrt(jnp.sum(total, axis=-1, keepdims=True) * (1.0 / D) + EPS)
        for b in range(8):
            columns = slice(b * 256, (b + 1) * 256)
            normed[rows, columns] = (middle[rows, columns].astype(F32) * scale * chan_row[:, columns]).astype(BF)

    base = 52.0
    at(base)
    gather(middle_view, "c", [base + t for t in gather_times], norm_block)
    norm_block(0, core)

    need(3)
    at(64.0)
    project(w_up, 256, keep_hidden)

    need(4)
    around = (2, 1, -1, 0)

    def terms(o, c):
        return turned_dot(hidden[...], w_down[pl.ds(pl.multiple_of(block_of(o, c) * 256, 256), 256), :])

    halves = (slice(0, 256), slice(256, 512))
    for n, o in enumerate(around):
        give2[n] = terms(o, 1 - core).astype(BF)
        send(give2.at[n], take2.at[n], "partner", ("d", n))

    def summed(n):
        arrive(take2.at[n], ("d", n))
        own2[...] = terms(around[n], core) + take2[n].astype(F32)

    summed(0)
    move2[0] = own2[halves[0], :].astype(BF)
    move2[1] = own2[halves[1], :].astype(BF)
    send(move2.at[0], pass2.at[0], "right", ("d2", 0))
    send(move2.at[1], pass2.at[1], "left", ("d2", 1))
    summed(1)
    move2[2] = own2[halves[1], :].astype(BF)
    move2[4] = own2[halves[0], :].astype(BF)
    send(move2.at[2], left2.at[halves[1]], "right", ("d1", 0))
    summed(2)
    move2[3] = own2[halves[0], :].astype(BF)
    move2[5] = own2[halves[1], :].astype(BF)
    send(move2.at[3], right2.at[halves[0]], "left", ("d1", 1))
    arrive(pass2.at[0], ("d2", 0))
    move2[4] = (move2[4].astype(F32) + pass2[0].astype(F32)).astype(BF)
    send(move2.at[4], left2.at[halves[0]], "right", ("d3", 0))
    arrive(pass2.at[1], ("d2", 1))
    move2[5] = (move2[5].astype(F32) + pass2[1].astype(F32)).astype(BF)
    send(move2.at[5], right2.at[halves[1]], "left", ("d3", 1))
    summed(3)
    own2[...] += middle[:, pl.ds(pl.multiple_of(tp * 256, 256), 256)].astype(F32)
    arrive(left2.at[halves[1]], ("d1", 0))
    arrive(right2.at[halves[0]], ("d1", 1))
    arrive(left2.at[halves[0]], ("d3", 0))
    arrive(right2.at[halves[1]], ("d3", 1))
    result[...] = (own2[...] + left2[...].astype(F32) + right2[...].astype(F32)).astype(BF)
    at(1000.0)
    for copy in sends:
        copy.wait_send()


def rotary_tables():
    half = DK // 2
    angle = np.arange(ROWS)[:, None] * THETA ** (-np.arange(half) / half)
    return np.cos(angle).astype(np.float32), np.sin(angle).astype(np.float32)


def shards(tokens, mix_gain, query_w, key_w, value_w, head_gain, out_w, chan_gain, up_w, down_w):
    cosine, sine = rotary_tables()
    any_place = pl.BlockSpec(memory_space=pl.ANY)
    vmem = pltpu.VMEM
    scratch = [
        *[vmem((D, 512), BF)] * 5,
        vmem((8, ROWS, 256), BF),
        vmem((ROWS, D), BF),
        vmem((ROWS, D), BF),
        vmem((2, 512, 64), BF),
        vmem((1, D), F32),
        vmem((1, D), F32),
        vmem((8, DV), F32),
        vmem((ROWS, DK // 2), F32),
        vmem((ROWS, DK // 2), F32),
        vmem((4, 128, 128), F32),
        vmem((ROWS, 512), F32),
        vmem((ROWS, DK), BF),
        vmem((ROWS, DK), BF),
        vmem((ROWS, DV), BF),
        vmem((4, 2, 64, DV), BF),
        vmem((ROWS, 512), BF),
        vmem((4, 256, 512), BF),
        vmem((4, 256, 512), BF),
        vmem((4, 256, 512), F32),
        vmem((4, 4, 32, 512), BF),
        vmem((4, 2, 32, 512), BF),
        vmem((4, 64, 512), BF),
        vmem((4, 64, 512), BF),
        vmem((4, 2, 32, 512), BF),
        vmem((4, ROWS, 256), BF),
        vmem((4, ROWS, 256), BF),
        vmem((ROWS, 256), F32),
        vmem((6, 256, 256), BF),
        vmem((ROWS, 256), BF),
        vmem((ROWS, 256), BF),
        vmem((2, 256, 256), BF),
        pltpu.SemaphoreType.DMA((12,)),
        pltpu.SemaphoreType.DMA((260,)),
        pltpu.SemaphoreType.DMA((260,)),
    ]
    return pl.pallas_call(
        layer_kernel,
        out_shape=jax.ShapeDtypeStruct((ROWS, 256), BF),
        in_specs=[any_place] * 12,
        out_specs=pl.BlockSpec(memory_space=pltpu.VMEM),
        scratch_shapes=scratch,
        compiler_params=pltpu.CompilerParams(
            collective_id=0, has_side_effects=True, vmem_limit_bytes=60 << 20
        ),
        name="layer",
    )(
        tokens, mix_gain.reshape(1, D), query_w, key_w, value_w, head_gain, out_w,
        chan_gain.reshape(1, D), up_w, down_w, jnp.asarray(cosine), jnp.asarray(sine),
    )


def solution(mesh):
    placed = (
        P(("rep", "fs"), "tp"),
        P(),
        P("fs", "tp"),
        P("fs", "tp"),
        P("fs", "tp"),
        P(),
        P("tp", "fs"),
        P(),
        P("fs", "tp"),
        P("tp", "fs"),
    )
    return jax.shard_map(
        shards, mesh=mesh, in_specs=placed, out_specs=P(("rep", "fs"), "tp"), check_vma=False
    )
```

```python
import heapq
from collections import defaultdict

import jax
import jax.numpy as jnp
import numpy as np
from jax import lax
from jax.experimental import pallas as pl
from jax.experimental.pallas import tpu as pltpu
from jax.sharding import PartitionSpec as P

ROWS = 512
D = 2048
DK = 256
DV = 512
EPS = 1e-06
HEAD_EPS = 0.05
THETA = 10000.0
NX, NY, NZ = 4, 8, 4
MESH = pl.DeviceIdType.MESH
BF, F32 = jnp.bfloat16, jnp.float32

PARTS = (
    (0, 0, 64, "A", 0, 0.0),
    (1, 0, 64, "B", 1, 0.0),
    (2, 0, 64, "A", 1, 1.0),
    (3, 0, 32, "A", 2, 2.5),
    (3, 32, 32, "B", 2, 2.5),
    (4, 0, 32, "A", 2, 2.5),
    (4, 32, 32, "B", 2, 2.5),
)
SENDS, LANDS = 13, 220
LEAD = {"y": 3.2, "z": 3.2, "x": 2.0}
XRANK = {(t, i): (i + 1.5 * k, k) for k, t in enumerate("mcd") for i in range(4)}
RATE = {"ring": 45.2e3, "partner": 600e3}
DELAY = {"early": 2.3, "late": 3.0, "x": 2.2, "partner": 1.1}


def onward(p, a, b):
    out = []
    two = lambda k: 1 if k % 2 == 0 else -1
    if PARTS[p][3] == "A":
        fw = 4 if p % 4 < 2 else 3
        if b == 0:
            if 0 <= a < fw:
                out.append(("y", 1))
            if 0 >= a > fw - 7:
                out.append(("y", -1))
            out += [("z", 1), ("z", -1)]
        elif abs(b) == 1 and two(a) == b:
            out.append(("z", b))
    else:
        fw = 4 if b % 2 == 0 else 3
        if a == 0:
            if b == 0:
                out += [("z", 1), ("z", -1)]
            elif abs(b) == 1 and two(p // 2) == b:
                out.append(("z", b))
        if 0 <= a < fw:
            out.append(("y", 1))
        if 0 >= a > fw - 7:
            out.append(("y", -1))
    return [(k, a + k[1] * (k[0] == "y"), b + k[1] * (k[0] == "z")) for k in out]


def below(p, a, b):
    return max([0] + [1 + below(p, na, nb) for _, na, nb in onward(p, a, b)])


def schedule(tasks, messages):
    left, users, leaving = {}, defaultdict(list), defaultdict(list)
    for name, (needs, _, _, start) in tasks.items():
        left[name] = len(needs) + 1
        for need in needs:
            users[need].append(name)
    for name, (task, *_) in messages.items():
        leaving[task].append(name)
    events, ready, items = [], [], []
    count = 0
    link_free = defaultdict(float)
    queue = defaultdict(list)
    core_free = 0.0
    for name, (_, _, _, start) in tasks.items():
        heapq.heappush(events, (start, count, "part", name))
        count += 1
    now = 0.0

    def serve(link, time):
        nonlocal count
        while queue[link] and link_free[link] <= time + 1e-9:
            message = heapq.heappop(queue[link])[-1]
            kind = "partner" if link == "partner" else "ring"
            begin = max(time, link_free[link])
            link_free[link] = begin + messages[message][2] / RATE[kind]
            if messages[message][3] is not None:
                items.append((max(available[message], begin - LEAD[link[0]]), 1, len(items), "send", message))
            rank = messages[message][3]
            delay = DELAY["partner" if link == "partner" else "x" if link[0] == "x" else "early" if rank[0] < 2 else "late"]
            heapq.heappush(events, (link_free[link] + delay, count, "arrive", message))
            heapq.heappush(events, (link_free[link], count + 1, "link", link))
            count += 2

    available, arrived, done = {}, {}, {}
    while events:
        now, _, kind, name = heapq.heappop(events)
        if kind == "link":
            serve(name, now)
        elif kind == "free":
            done[name] = now
            for message in leaving[name]:
                task, link, size, rank = messages[message]
                available[message] = now
                heapq.heappush(queue[link], ((99, now) if rank is None else rank, count, message))
                count += 1
                serve(link, now)
        targets = [name] if kind == "part" else users[name] if kind in ("arrive", "free") else []
        if kind == "arrive":
            arrived[name] = now
        for task in targets:
            left[task] -= 1
            if left[task] == 0:
                heapq.heappush(ready, (tasks[task][2], count, task))
                count += 1
        while ready and core_free <= now + 1e-9:
            if events and events[0][0] <= now + 1e-9 and events[0][2] != "link":
                break
            task = heapq.heappop(ready)[-1]
            items.append((now, 0, len(items), "task", task))
            core_free = now + tasks[task][1]
            heapq.heappush(events, (core_free, count, "free", task))
            count += 1
    assert len(done) == len(tasks), "cycle"
    items.sort()
    sent = set()
    for _, _, _, kind, name in items:
        if kind == "send":
            sent.add(name)
        else:
            assert all(n in done or n in sent for n in tasks[name][0]), "order"
            sent.update(m for m in leaving[name] if messages[m][3] is None)
    return items, done


def turned_dot(left, right):
    return lax.dot_general(left, right, (((1,), (1,)), ((), ())), preferred_element_type=F32)


def layer_kernel(
    tokens, mix_gain, query_w, key_w, value_w, head_gain, out_w, chan_gain, up_w, down_w, cosine, sine,
    result,
    w_both, w_value, w_out, w_up, w_down, down_turned,
    blocks, normed, middle, mix_row, chan_row, head_rows, cos_tab, sin_tab, decay,
    raw, raw_value, query, keys, values, head_out, hidden,
    terms1, give1, take1, move1, left1, right1, pass1,
    terms2, give2, take2, move2, left2, right2, pass2,
    local_sem, send_sem, recv_sem,
):
    rep, fs, tp = lax.axis_index("rep"), lax.axis_index("fs"), lax.axis_index("tp")
    z, y = fs // NY, fs % NY
    x, core = tp // 2, tp % 2
    units = (w_both, w_value, w_out, w_up, w_down)
    target = {
        ("y", 1): {"fs": z * NY + (y + 1) % NY},
        ("y", -1): {"fs": z * NY + (y + NY - 1) % NY},
        ("z", 1): {"rep": (rep + (z + 1) // NZ) % 2, "fs": ((z + 1) % NZ) * NY + y},
        ("z", -1): {"rep": (rep + (NZ - z) // NZ) % 2, "fs": ((z + NZ - 1) % NZ) * NY + y},
        ("x", 1): {"tp": ((x + 1) % NX) * 2 + core},
        ("x", -1): {"tp": ((x + NX - 1) % NX) * 2 + core},
        "partner": {"tp": x * 2 + (1 - core)},
    }
    barrier = pltpu.get_barrier_semaphore()
    for k in target:
        pl.semaphore_signal(barrier, inc=1, device_id=target[k], device_id_type=MESH)

    def slot(a, b):
        at = ((z - b + NZ) % NZ) * NY + (y - a + NY) % NY
        return pl.ds(pl.multiple_of(at * 64, 64), 64)

    mine = slot(0, 0)
    local = []

    def bring(source, dest):
        copy = pltpu.make_async_copy(source, dest, local_sem.at[len(local)])
        copy.start()
        local.append(copy)

    bring(tokens, blocks.at[tp])
    bring(query_w, w_both.at[mine, 0:DK])
    bring(key_w, w_both.at[mine, DK : 2 * DK])
    bring(value_w, w_value.at[mine])
    bring(out_w, w_out.at[mine])
    bring(up_w, w_up.at[mine])
    bring(down_w, w_down.at[mine])
    bring(mix_gain, mix_row)
    bring(chan_gain, chan_row)
    bring(head_gain, head_rows)
    bring(cosine, cos_tab)
    bring(sine, sin_tab)
    for copy in local[:4]:
        copy.wait()
    pl.semaphore_wait(barrier, len(target))

    tasks, bodies = {}, {}
    messages, views = {}, {}
    lands, leaves, totals = {}, {}, {}

    def task(name, needs, cost, rank, body=None, start=0.0):
        tasks[name] = (needs, cost, rank, start)
        bodies[name] = body

    def message(name, after, link, size, source, dest, here, rank=None, share=None, sent=None):
        messages[name] = (after, link, size, rank)
        views[name] = (source, dest, share[1] if share else here)
        lands[name] = share[0] if share else name
        leaves[name] = sent[0]
        totals[sent[0]] = sent[1]

    def piece(p, a, b):
        u, first, count = PARTS[p][:3]
        at = ((z - b + NZ) % NZ) * NY + (y - a + NY) % NY
        return units[u].at[pl.ds(pl.multiple_of(at * 64 + first, 16), count)]

    inside = defaultdict(list)
    for p, (u, _, count, _, rank, start) in enumerate(PARTS):
        stack, ends = [(0, 0)], defaultdict(list)
        sent = (("w", p), units[u].at[pl.ds(0, 31 * count)])
        seen = {}
        while stack:
            a, b = stack.pop()
            seen[a, b] = onward(p, a, b)
            if not seen[a, b]:
                ends[2 if abs(b) == 2 else b].append((a, b))
            stack += [(na, nb) for _, na, nb in seen[a, b]]
        for (a, b), following in seen.items():
            if not following:
                continue
            name = ("w", p, a, b)
            needs = ([] if u < 2 else ["prepare"]) if (a, b) == (0, 0) else [name]
            task(("got", *name), needs, 0.02, -1, None, start)
            inside[u].append(("got", *name))
            for k, na, nb in following:
                group = [(g, e) for g, e in ends.items() if (na, nb) in e]
                share = None
                if group:
                    share = (("end", p, group[0][0]), units[u].at[pl.ds(0, len(group[0][1]) * count)])
                message(
                    ("w", p, na, nb), ("got", *name), k, count * 1024,
                    piece(p, a, b), piece(p, a, b), piece(p, na, nb), (rank, -1 - below(p, na, nb)), share, sent,
                )
        for g, group in ends.items():
            name = ("got", "w", p, "end", g)
            task(name, [("w", p, a, b) for a, b in group], 0.02, 1, None)
            inside[u].append(name)

    planes = (0, 1, -1, 2)

    def plane(b):
        return (z - b + NZ) % NZ

    def of_plane(u, b):
        return [n for n in inside[u] if n[-1] in ((2, -2) if b == 2 else (b,))]

    def plane_rows(b):
        return pl.ds(pl.multiple_of(plane(b) * 512, 512), 512)

    def turn(b):
        at = pl.multiple_of(plane(b) * 512, 512)
        for n in range(4):
            down_turned[:, pl.ds(at + n * 128, 128)] = w_down[pl.ds(at + n * 128, 128), :].T

    for b in planes:
        task(("turn", b), of_plane(4, b), 0.22, 2, lambda b=b: turn(b))
    turned = [("turn", b) for b in planes]

    def at_x(o):
        return (x + o + NX) % NX

    def gather(tag, view, size, first, needs, rank, ref, sent):
        task((tag, 0, 0), needs, 0.01 if first is None else first[0], 0, first and first[1])
        parts = [(0, 0), (-1, 0), (1, 1), (-1, 1), (1, 0), (-2, 0), (2, 1)]
        for o, h in parts[1:]:
            task((tag, o, h), [(tag, "m", o, h)], 0.02, 0)
        task((tag, "p"), [(tag, "mp", o, h) for o, h in parts + [(0, 1)]], 0.02, 1)

        def pass_on(o, h, after, link, no):
            message((tag, "m", no, h), after, link, size, view(o, core, h), view(o, core, h), view(no, core, h), (*rank, 0 if no in (-2, 2) else 1), None, sent)

        pass_on(0, 0, (tag, 0, 0), ("x", 1), -1)
        pass_on(0, 1, (tag, 0, 0), ("x", -1), 1)
        pass_on(0, 1, (tag, 0, 0), ("x", 1), -1)
        pass_on(0, 0, (tag, 0, 0), ("x", -1), 1)
        pass_on(-1, 0, (tag, -1, 0), ("x", 1), -2)
        pass_on(1, 1, (tag, 1, 1), ("x", -1), 2)
        for o, h in parts + [(0, 1)]:
            after = (tag, 0, 0) if o == 0 else (tag, o, h)
            message(
                (tag, "mp", o, h), after, "partner", size,
                view(o, core, h), view(o, core, h), view(o, 1 - core, h), None, ((tag, "p"), ref), sent,
            )
        return [(tag, o, h) for o, h in parts] + [(tag, "p")]

    def token_view(o, c, h):
        return blocks.at[at_x(o) * 2 + c, pl.ds(h * 256, 256)]

    all_tokens = gather("t", token_view, 131072, None, [], (0, 0), blocks.at[pl.ds(0, 4)], ("t", blocks.at[pl.ds(0, 7)]))

    def prepare():
        for copy in local[4:]:
            copy.wait()
        rate = jnp.float32(0.0)
        for h in range(8):
            rate = jnp.where(tp == h, jnp.float32(np.log1p(-(2.0 ** (-5 - h)))), rate)
        offset = (
            lax.broadcasted_iota(jnp.int32, (128, 128), 0) - lax.broadcasted_iota(jnp.int32, (128, 128), 1)
        ).astype(F32)
        for n in range(4):
            value = jnp.exp(rate * jnp.maximum(offset + 128.0 * n, 0.0))
            decay[n] = jnp.where(offset + 128.0 * n >= 0, value, 0.0)

    task("prepare", [], 0.4, -2, prepare, 0.5)

    def scaled(dest, read, gain, rows):
        total = jnp.zeros((64, 256), F32)
        for b in range(8):
            part = read(b, rows).astype(F32)
            total = total + part * part
        scale = lax.rsqrt(jnp.sum(total, axis=-1, keepdims=True) * (1.0 / D) + EPS)
        for b in range(8):
            columns = slice(b * 256, (b + 1) * 256)
            dest[rows, columns] = (read(b, rows).astype(F32) * scale * gain[:, columns]).astype(BF)

    def norm_tokens(n):
        @pl.loop(0, 4)
        def _(i):
            rows = pl.ds(pl.multiple_of(n * 256 + i * 64, 64), 64)
            scaled(normed, lambda b, r: blocks[b, r, :], mix_row, rows)

    for n in range(2):
        task(("norm", n), all_tokens + ["prepare"], 0.65, 2, lambda n=n: norm_tokens(n))

    def columns_of(n):
        return slice(n * 256, (n + 1) * 256)

    def project(weights, dest, b):
        at = plane_rows(b)

        @pl.loop(0, 2)
        def _(n):
            columns = pl.ds(pl.multiple_of(n * 256, 256), 256)
            value = jnp.dot(normed[:, at], weights[at, columns], preferred_element_type=F32)
            dest[:, columns] = value if b == 0 else dest[:, columns] + value

    def round_values():
        values[...] = raw_value[...].astype(BF)

    def rotary():
        @pl.loop(0, ROWS // 64)
        def _(i):
            rows = pl.ds(pl.multiple_of(i * 64, 64), 64)
            c, s = cos_tab[rows, :], sin_tab[rows, :]
            for start, dest, factor in ((0, query, 1.0), (DK, keys, DK**-0.5)):
                first, second = raw[rows, start : start + 128], raw[rows, start + 128 : start + 256]
                dest[rows, 0:128] = ((first * c - second * s) * factor).astype(BF)
                dest[rows, 128:256] = ((second * c + first * s) * factor).astype(BF)

    before = [("norm", 0), ("norm", 1)]
    for u, dest, name in ((0, raw, "both"), (1, raw_value, "value")):
        last = []
        for b in planes:
            task(
                (name, b), of_plane(u, b) + before + last, 0.6, 3,
                lambda u=u, dest=dest, b=b: project(units[u], dest, b),
            )
            last = [(name, b)]
    task("rotary", [("both", 2)], 0.25, 3, rotary)
    task("values", [("value", 2)], 0.1, 3, round_values)

    def retain(i):
        gain = head_rows[pl.ds(tp, 1), :]
        rows = slice(i * 128, (i + 1) * 128)
        total = jnp.zeros((128, DV), F32)
        for j in range(i + 1):
            there = slice(j * 128, (j + 1) * 128)
            score = turned_dot(query[rows, :], keys[there, :]) * decay[i - j]
            total = total + jnp.dot(score.astype(BF), values[there, :], preferred_element_type=F32)
        scale = lax.rsqrt(jnp.mean(total * total, axis=-1, keepdims=True) + HEAD_EPS)
        head_out[rows, :] = (total * scale * gain).astype(BF)

    for i in range(4):
        task(("retain", i), ["rotary", "values"], 0.4 + 0.1 * i, 3, lambda i=i: retain(i))

    def reduce(tag, i, needs, cost, compute, buffers, part, half, size, settle, settle_cost):
        give, take, move, left, right, through = buffers
        task((tag, "terms", i), needs, cost, 3 + i, compute)
        message(
            (tag, "give", i), (tag, "terms", i), "partner", 8 * size, give.at[i], take.at[i], take.at[i],
            None, None, ((tag, "give"), give),
        )

        def spread():
            for n, (o, h) in enumerate(((2, 0), (2, 1), (1, 1), (-1, 0))):
                move[i, n] = part(i, o, h).astype(BF)

        task((tag, "spread", i), [(tag, "give", i)], 0.1, 1, spread)
        for n, (link, dest) in enumerate(
            (
                (("x", 1), through.at[i, 0]),
                (("x", -1), through.at[i, 1]),
                (("x", 1), left.at[(i, *half(1))]),
                (("x", -1), right.at[(i, *half(0))]),
                (("x", 1), left.at[(i, *half(0))]),
                (("x", -1), right.at[(i, *half(1))]),
            )
        ):
            after = (tag, "spread", i) if n < 4 else (tag, "merge", i, n - 4)
            message((tag, "move", i, n), after, link, size, move.at[i, n], dest, dest, (*XRANK[tag, i], (1, 1, 2, 2, 0, 0)[n]),
                None if n < 2 else ((tag, "last", i), move.at[i, pl.ds(0, 4)]), ((tag, "move"), move))

        def merge(h):
            o = 1 if h == 0 else -1
            move[i, 4 + h] = (part(i, o, h) + through[i, h].astype(F32)).astype(BF)

        for h in range(2):
            task(
                (tag, "merge", i, h), [(tag, "move", i, h), (tag, "spread", i)], 0.06, 0, lambda h=h: merge(h)
            )
        needs = [(tag, "spread", i)] + [(tag, "move", i, n) for n in range(2, 6)]
        return needs, settle_cost, settle

    def half1(h):
        return (slice(h * 32, (h + 1) * 32), slice(None))

    def part1(i, o, h):
        rows, columns = half1(h)
        return terms1[i, core, at_x(o), rows, columns] + take1[i, at_x(o), rows, columns].astype(F32)

    def out_terms(i):
        at = pl.multiple_of(plane(planes[i]) * 512, 512)
        for n in range(2):
            value = turned_dot(head_out[...], w_out[pl.ds(at + n * 256, 256), :])
            terms1[i, :, :, :, columns_of(n)] = value.reshape(2, 4, 64, 256)
        give1[i] = terms1[i, 1 - core].astype(BF)

    def token_rows(o, c, h=None):
        start, size = (0, 64) if h is None else (h * 32, 32)
        return pl.ds(pl.multiple_of(c * 256 + at_x(o) * 64 + start, size), size)

    def settle1(i):
        p = plane(planes[i])
        rows = token_rows(0, core)
        total = terms1[i, core, x] + take1[i, x].astype(F32) + left1[i].astype(F32) + right1[i].astype(F32)
        for n in range(2):
            middle[p, rows, columns_of(n)] = (total[:, columns_of(n)] + blocks[2 * p + n, rows, :].astype(F32)).astype(BF)

    def middle_view(i):
        return lambda o, c, h: middle.at[plane(planes[i]), token_rows(o, c, h)]

    def norm_middle(i):
        @pl.loop(0, 2)
        def _(n):
            rows = pl.ds(pl.multiple_of(i * 128 + n * 64, 64), 64)
            scaled(normed, lambda b, r: middle[b // 2, r, columns_of(b % 2)], chan_row, rows)

    def mix_up(i):
        rows = slice(i * 128, (i + 1) * 128)
        for n in range(2):
            value = jnp.maximum(
                jnp.dot(normed[rows, :], w_up[:, columns_of(n)], preferred_element_type=F32), 0.0
            )
            hidden[rows, columns_of(n)] = (value * value).astype(BF)

    def half2(h):
        return (slice(h * 64, (h + 1) * 64), slice(None))

    def part2(i, o, h):
        rows, columns = half2(h)
        return terms2[i, at_x(o), core, rows, columns] + take2[i, at_x(o), rows, columns].astype(F32)

    def down_terms(i):
        rows = slice(i * 128, (i + 1) * 128)

        for n in range(8):
            value = jnp.dot(hidden[rows, :], down_turned[:, columns_of(n)], preferred_element_type=F32)
            terms2[i, n // 2, n % 2] = value

        for n in range(4):
            give2[i, n] = terms2[i, n, 1 - core].astype(BF)

    def settle2(i):
        rows = slice(i * 128, (i + 1) * 128)
        total = terms2[i, x, core] + take2[i, x].astype(F32)
        total = total + left2[i].astype(F32) + right2[i].astype(F32)
        columns = pl.ds(pl.multiple_of(core * 256, 256), 256)
        result[rows, :] = total + middle[x, rows, columns].astype(F32)

    pieces = []
    for i, b in enumerate(planes):
        needs, cost, body = reduce(
            "m", i, of_plane(2, b) + [("retain", n) for n in range(4)], 0.5, lambda i=i: out_terms(i),
            (give1, take1, move1, left1, right1, pass1), part1, half1, 32768, lambda i=i: settle1(i), 0.08,
        )
        pieces += gather(
            ("c", i), middle_view(i), 32768, (cost, body), needs, XRANK["c", i],
            middle.at[0, pl.ds(0, 256)], ("c", middle.at[:, pl.ds(0, 448)]),
        )
    for i in range(4):
        task(("norm2", i), pieces + [("both", 2), ("value", 2)], 0.32, 3 + i, lambda i=i: norm_middle(i))
        task(("up", i), inside[3] + [("norm2", i)], 0.45, 3 + i, lambda i=i: mix_up(i))
        needs, cost, body = reduce(
            "d", i, turned + [("up", i)], 0.52, lambda i=i: down_terms(i),
            (give2, take2, move2, left2, right2, pass2), part2, half2, 32768, lambda i=i: settle2(i), 0.08,
        )
        task(("last", i), needs, cost, 1, body)

    items, _ = schedule(tasks, messages)
    number = {n: k for k, n in enumerate(dict.fromkeys(lands.values()))}
    sender = {n: k for k, n in enumerate(totals)}
    assert len(number) <= LANDS and len(sender) <= SENDS, "semaphores"

    def start(name):
        source, dest, _ = views[name]
        copy = pltpu.make_async_remote_copy(
            src_ref=source,
            dst_ref=dest,
            send_sem=send_sem.at[sender[leaves[name]]],
            recv_sem=recv_sem.at[number[lands[name]]],
            device_id=target[messages[name][1]],
            device_id_type=MESH,
        )
        copy.start()

    departing = defaultdict(list)
    for name, (after, _, _, rank) in messages.items():
        if rank is None:
            departing[after].append(name)
    for _, _, _, kind, name in items:
        if kind == "send":
            start(name)
            continue
        waits = [n for n in tasks[name][0] if n in messages]
        if waits:
            for key in dict.fromkeys(lands[n] for n in waits):
                here = next(views[n][2] for n in waits if lands[n] == key)
                pltpu.make_async_copy(here, here, recv_sem.at[number[key]]).wait()
        if bodies[name]:
            bodies[name]()
        for n in departing[name]:
            start(n)
    for key, whole in totals.items():
        pltpu.make_async_copy(whole, whole, send_sem.at[sender[key]]).wait()


def rotary_tables():
    half = DK // 2
    angle = np.arange(ROWS)[:, None] * THETA ** (-np.arange(half) / half)
    return np.cos(angle).astype(np.float32), np.sin(angle).astype(np.float32)


def shards(tokens, mix_gain, query_w, key_w, value_w, head_gain, out_w, chan_gain, up_w, down_w):
    cosine, sine = rotary_tables()
    any_place = pl.BlockSpec(memory_space=pl.ANY)
    vmem = pltpu.VMEM
    scratch = [
        *[vmem((D, 512), BF)] * 5,
        vmem((512, D), BF),
        vmem((8, ROWS, 256), BF),
        vmem((ROWS, D), BF),
        vmem((4, ROWS, 512), BF),
        vmem((1, D), F32),
        vmem((1, D), F32),
        vmem((8, DV), F32),
        vmem((ROWS, DK // 2), F32),
        vmem((ROWS, DK // 2), F32),
        vmem((4, 128, 128), F32),
        vmem((ROWS, 512), F32),
        vmem((ROWS, 512), F32),
        vmem((ROWS, DK), BF),
        vmem((ROWS, DK), BF),
        vmem((ROWS, DV), BF),
        vmem((ROWS, DV), BF),
        vmem((ROWS, 512), BF),
        vmem((4, 2, 4, 64, 512), F32),
        vmem((4, 4, 64, 512), BF),
        vmem((4, 4, 64, 512), BF),
        vmem((4, 6, 32, 512), BF),
        vmem((4, 64, 512), BF),
        vmem((4, 64, 512), BF),
        vmem((4, 2, 32, 512), BF),
        vmem((4, 4, 2, 128, 256), F32),
        vmem((4, 4, 128, 256), BF),
        vmem((4, 4, 128, 256), BF),
        vmem((4, 6, 64, 256), BF),
        vmem((4, 128, 256), BF),
        vmem((4, 128, 256), BF),
        vmem((4, 2, 64, 256), BF),
        pltpu.SemaphoreType.DMA((12,)),
        pltpu.SemaphoreType.DMA((SENDS,)),
        pltpu.SemaphoreType.DMA((LANDS,)),
    ]
    whole = pl.pallas_call(
        layer_kernel,
        out_shape=jax.ShapeDtypeStruct((ROWS, 256), F32),
        in_specs=[any_place] * 12,
        out_specs=pl.BlockSpec(memory_space=pltpu.VMEM),
        scratch_shapes=scratch,
        compiler_params=pltpu.CompilerParams(
            collective_id=0, has_side_effects=True, vmem_limit_bytes=60 << 20
        ),
        name="layer",
    )(
        tokens, mix_gain.reshape(1, D), query_w, key_w, value_w, head_gain, out_w.T,
        chan_gain.reshape(1, D), up_w, down_w.T, jnp.asarray(cosine), jnp.asarray(sine),
    )
    return whole.astype(BF)


def solution(mesh):
    placed = (
        P(("rep", "fs"), "tp"),
        P(),
        P("fs", "tp"),
        P("fs", "tp"),
        P("fs", "tp"),
        P(),
        P("tp", "fs"),
        P(),
        P("fs", "tp"),
        P("tp", "fs"),
    )
    return jax.shard_map(
        shards, mesh=mesh, in_specs=placed, out_specs=P(("rep", "fs"), "tp"), check_vma=False
    )
```

```python
import heapq
from collections import defaultdict

import jax
import jax.numpy as jnp
import numpy as np
from jax import lax
from jax.experimental import pallas as pl
from jax.experimental.pallas import tpu as pltpu
from jax.sharding import PartitionSpec as P

ROWS = 512
D = 2048
DK = 256
DV = 512
EPS = 1e-06
HEAD_EPS = 0.05
THETA = 10000.0
NX, NY, NZ = 4, 8, 4
MESH = pl.DeviceIdType.MESH
BF, F32 = jnp.bfloat16, jnp.float32

PARTS = (
    (0, 0, 64, "A", 0, 0.0),
    (1, 0, 64, "B", 1, 0.0),
    (2, 0, 64, "A", 1, 1.0),
    (3, 0, 32, "A", 2, 2.5),
    (3, 32, 32, "B", 2, 2.5),
    (4, 0, 32, "A", 2, 2.5),
    (4, 32, 32, "B", 2, 2.5),
)
SENDS, LANDS = 13, 220
LEAD = {"y": 1.5, "z": 1.5, "x": 1.2}
XRANK = {(t, i): (i + 1.5 * k, k) for k, t in enumerate("mcd") for i in range(4)}
RATE = {"ring": 45.2e3, "partner": 600e3}
DELAY = {"early": 2.3, "late": 2.5, "x": 2.2, "partner": 1.1}


def onward(p, a, b):
    out = []
    two = lambda k: 1 if k % 2 == 0 else -1
    if PARTS[p][3] == "A":
        fw = 4 if p % 4 < 2 else 3
        if b == 0:
            if 0 <= a < fw:
                out.append(("y", 1))
            if 0 >= a > fw - 7:
                out.append(("y", -1))
            out += [("z", 1), ("z", -1)]
        elif abs(b) == 1 and two(a) == b:
            out.append(("z", b))
    else:
        fw = 4 if b % 2 == 0 else 3
        if a == 0:
            if b == 0:
                out += [("z", 1), ("z", -1)]
            elif abs(b) == 1 and two(p // 2) == b:
                out.append(("z", b))
        if 0 <= a < fw:
            out.append(("y", 1))
        if 0 >= a > fw - 7:
            out.append(("y", -1))
    return [(k, a + k[1] * (k[0] == "y"), b + k[1] * (k[0] == "z")) for k in out]


def below(p, a, b):
    return max([0] + [1 + below(p, na, nb) for _, na, nb in onward(p, a, b)])


def schedule(tasks, messages):
    left, users, leaving = {}, defaultdict(list), defaultdict(list)
    for name, (needs, _, _, start) in tasks.items():
        left[name] = len(needs) + 1
        for need in needs:
            users[need].append(name)
    for name, (task, *_) in messages.items():
        leaving[task].append(name)
    events, ready, items = [], [], []
    count = 0
    link_free = defaultdict(float)
    queue = defaultdict(list)
    core_free = 0.0
    for name, (_, _, _, start) in tasks.items():
        heapq.heappush(events, (start, count, "part", name))
        count += 1
    now = 0.0

    def serve(link, time):
        nonlocal count
        while queue[link] and link_free[link] <= time + 1e-9:
            message = heapq.heappop(queue[link])[-1]
            kind = "partner" if link == "partner" else "ring"
            begin = max(time, link_free[link])
            link_free[link] = begin + messages[message][2] / RATE[kind]
            if messages[message][3] is not None:
                items.append((max(available[message], begin - LEAD[link[0]]), 1, len(items), "send", message))
            rank = messages[message][3]
            delay = DELAY["partner" if link == "partner" else "x" if link[0] == "x" else "early" if rank[0] < 2 else "late"]
            heapq.heappush(events, (link_free[link] + delay, count, "arrive", message))
            heapq.heappush(events, (link_free[link], count + 1, "link", link))
            count += 2

    available, arrived, done = {}, {}, {}
    while events:
        now, _, kind, name = heapq.heappop(events)
        if kind == "link":
            serve(name, now)
        elif kind == "free":
            done[name] = now
            for message in leaving[name]:
                task, link, size, rank = messages[message]
                available[message] = now
                heapq.heappush(queue[link], ((99, now) if rank is None else rank, count, message))
                count += 1
                serve(link, now)
        targets = [name] if kind == "part" else users[name] if kind in ("arrive", "free") else []
        if kind == "arrive":
            arrived[name] = now
        for task in targets:
            left[task] -= 1
            if left[task] == 0:
                heapq.heappush(ready, (tasks[task][2], count, task))
                count += 1
        while ready and core_free <= now + 1e-9:
            if events and events[0][0] <= now + 1e-9 and events[0][2] != "link":
                break
            task = heapq.heappop(ready)[-1]
            items.append((now, 0, len(items), "task", task))
            core_free = now + tasks[task][1]
            heapq.heappush(events, (core_free, count, "free", task))
            count += 1
    assert len(done) == len(tasks), "cycle"
    items.sort()
    sent = set()
    for _, _, _, kind, name in items:
        if kind == "send":
            sent.add(name)
        else:
            assert all(n in done or n in sent for n in tasks[name][0]), "order"
            sent.update(m for m in leaving[name] if messages[m][3] is None)
    return items, done


def turned_dot(left, right):
    return lax.dot_general(left, right, (((1,), (1,)), ((), ())), preferred_element_type=F32)


def layer_kernel(
    tokens, mix_gain, query_w, key_w, value_w, head_gain, out_w, chan_gain, up_w, down_w, cosine, sine,
    result,
    w_both, w_value, w_out, w_up, w_down, down_turned,
    blocks, normed, middle, mix_row, chan_row, head_rows, cos_tab, sin_tab, decay,
    raw, raw_value, query, keys, values, head_out, hidden,
    terms1, give1, take1, move1, left1, right1, pass1,
    terms2, give2, take2, move2, left2, right2, pass2,
    answer, local_sem, send_sem, recv_sem,
):
    rep, fs, tp = lax.axis_index("rep"), lax.axis_index("fs"), lax.axis_index("tp")
    z, y = fs // NY, fs % NY
    x, core = tp // 2, tp % 2
    units = (w_both, w_value, w_out, w_up, w_down)
    target = {
        ("y", 1): {"fs": z * NY + (y + 1) % NY},
        ("y", -1): {"fs": z * NY + (y + NY - 1) % NY},
        ("z", 1): {"rep": (rep + (z + 1) // NZ) % 2, "fs": ((z + 1) % NZ) * NY + y},
        ("z", -1): {"rep": (rep + (NZ - z) // NZ) % 2, "fs": ((z + NZ - 1) % NZ) * NY + y},
        ("x", 1): {"tp": ((x + 1) % NX) * 2 + core},
        ("x", -1): {"tp": ((x + NX - 1) % NX) * 2 + core},
        "partner": {"tp": x * 2 + (1 - core)},
    }
    barrier = pltpu.get_barrier_semaphore()
    for k in target:
        pl.semaphore_signal(barrier, inc=1, device_id=target[k], device_id_type=MESH)

    def slot(a, b):
        at = ((z - b + NZ) % NZ) * NY + (y - a + NY) % NY
        return pl.ds(pl.multiple_of(at * 64, 64), 64)

    mine = slot(0, 0)
    local = []

    def bring(source, dest):
        copy = pltpu.make_async_copy(source, dest, local_sem.at[len(local)])
        copy.start()
        local.append(copy)

    bring(tokens, blocks.at[tp])
    bring(query_w, w_both.at[mine, 0:DK])
    bring(key_w, w_both.at[mine, DK : 2 * DK])
    bring(value_w, w_value.at[mine])
    bring(out_w, w_out.at[mine])
    bring(up_w, w_up.at[mine])
    bring(down_w, w_down.at[mine])
    bring(mix_gain, mix_row)
    bring(chan_gain, chan_row)
    bring(head_gain, head_rows)
    bring(cosine, cos_tab)
    bring(sine, sin_tab)
    for copy in local[:4]:
        copy.wait()
    pl.semaphore_wait(barrier, len(target))

    tasks, bodies = {}, {}
    messages, views = {}, {}
    lands, leaves, totals = {}, {}, {}

    def task(name, needs, cost, rank, body=None, start=0.0):
        tasks[name] = (needs, cost, rank, start)
        bodies[name] = body

    def message(name, after, link, size, source, dest, here, rank=None, share=None, sent=None):
        messages[name] = (after, link, size, rank)
        views[name] = (source, dest, share[1] if share else here)
        lands[name] = share[0] if share else name
        leaves[name] = sent[0]
        totals[sent[0]] = sent[1]

    def piece(p, a, b):
        u, first, count = PARTS[p][:3]
        at = ((z - b + NZ) % NZ) * NY + (y - a + NY) % NY
        return units[u].at[pl.ds(pl.multiple_of(at * 64 + first, 16), count)]

    inside = defaultdict(list)
    for p, (u, _, count, _, rank, start) in enumerate(PARTS):
        stack, ends = [(0, 0)], defaultdict(list)
        sent = (("w", p), units[u].at[pl.ds(0, 31 * count)])
        seen = {}
        while stack:
            a, b = stack.pop()
            seen[a, b] = onward(p, a, b)
            if not seen[a, b]:
                ends[2 if abs(b) == 2 else b].append((a, b))
            stack += [(na, nb) for _, na, nb in seen[a, b]]
        for (a, b), following in seen.items():
            if not following:
                continue
            name = ("w", p, a, b)
            needs = ([] if u < 2 else ["prepare"]) if (a, b) == (0, 0) else [name]
            task(("got", *name), needs, 0.02, -1, None, start)
            inside[u].append(("got", *name))
            for k, na, nb in following:
                group = [(g, e) for g, e in ends.items() if (na, nb) in e]
                share = None
                if group:
                    share = (("end", p, group[0][0]), units[u].at[pl.ds(0, len(group[0][1]) * count)])
                message(
                    ("w", p, na, nb), ("got", *name), k, count * 1024,
                    piece(p, a, b), piece(p, a, b), piece(p, na, nb), (rank, -1 - below(p, na, nb)), share, sent,
                )
        for g, group in ends.items():
            name = ("got", "w", p, "end", g)
            task(name, [("w", p, a, b) for a, b in group], 0.02, 1, None)
            inside[u].append(name)

    planes = (0, 1, -1, 2)

    def plane(b):
        return (z - b + NZ) % NZ

    def of_plane(u, b):
        return [n for n in inside[u] if n[-1] in ((2, -2) if b == 2 else (b,))]

    def plane_rows(b):
        return pl.ds(pl.multiple_of(plane(b) * 512, 512), 512)

    def turn(b):
        at = pl.multiple_of(plane(b) * 512, 512)
        for n in range(4):
            down_turned[:, pl.ds(at + n * 128, 128)] = w_down[pl.ds(at + n * 128, 128), :].T

    for b in planes:
        task(("turn", b), of_plane(4, b), 0.22, 2, lambda b=b: turn(b))
    turned = [("turn", b) for b in planes]

    def at_x(o):
        return (x + o + NX) % NX

    def gather(tag, view, size, first, needs, rank, ref, sent):
        task((tag, 0, 0), needs, 0.01 if first is None else first[0], 0, first and first[1])
        parts = [(0, 0), (-1, 0), (1, 1), (-1, 1), (1, 0), (-2, 0), (2, 1)]
        for o, h in parts[1:]:
            task((tag, o, h), [(tag, "m", o, h)], 0.02, 0)
        task((tag, "p"), [(tag, "mp", o, h) for o, h in parts + [(0, 1)]], 0.02, 1)

        def pass_on(o, h, after, link, no):
            message((tag, "m", no, h), after, link, size, view(o, core, h), view(o, core, h), view(no, core, h), (*rank, 0 if no in (-2, 2) else 1), None, sent)

        pass_on(0, 0, (tag, 0, 0), ("x", 1), -1)
        pass_on(0, 1, (tag, 0, 0), ("x", -1), 1)
        pass_on(0, 1, (tag, 0, 0), ("x", 1), -1)
        pass_on(0, 0, (tag, 0, 0), ("x", -1), 1)
        pass_on(-1, 0, (tag, -1, 0), ("x", 1), -2)
        pass_on(1, 1, (tag, 1, 1), ("x", -1), 2)
        for o, h in parts + [(0, 1)]:
            after = (tag, 0, 0) if o == 0 else (tag, o, h)
            message(
                (tag, "mp", o, h), after, "partner", size,
                view(o, core, h), view(o, core, h), view(o, 1 - core, h), None, ((tag, "p"), ref), sent,
            )
        return [(tag, o, h) for o, h in parts] + [(tag, "p")]

    def token_view(o, c, h):
        return blocks.at[at_x(o) * 2 + c, pl.ds(h * 256, 256)]

    all_tokens = gather("t", token_view, 131072, None, [], (0, 0), blocks.at[pl.ds(0, 4)], ("t", blocks.at[pl.ds(0, 7)]))

    def prepare():
        for copy in local[4:]:
            copy.wait()
        rate = jnp.float32(0.0)
        for h in range(8):
            rate = jnp.where(tp == h, jnp.float32(np.log1p(-(2.0 ** (-5 - h)))), rate)
        offset = (
            lax.broadcasted_iota(jnp.int32, (128, 128), 0) - lax.broadcasted_iota(jnp.int32, (128, 128), 1)
        ).astype(F32)
        for n in range(4):
            value = jnp.exp(rate * jnp.maximum(offset + 128.0 * n, 0.0))
            decay[n] = jnp.where(offset + 128.0 * n >= 0, value, 0.0)

    task("prepare", [], 0.4, -2, prepare, 0.5)

    def scaled(dest, read, gain, rows):
        total = jnp.zeros((64, 256), F32)
        for b in range(8):
            part = read(b, rows).astype(F32)
            total = total + part * part
        scale = lax.rsqrt(jnp.sum(total, axis=-1, keepdims=True) * (1.0 / D) + EPS)
        for b in range(8):
            columns = slice(b * 256, (b + 1) * 256)
            dest[rows, columns] = (read(b, rows).astype(F32) * scale * gain[:, columns]).astype(BF)

    def norm_tokens(n):
        @pl.loop(0, 4)
        def _(i):
            rows = pl.ds(pl.multiple_of(n * 256 + i * 64, 64), 64)
            scaled(normed, lambda b, r: blocks[b, r, :], mix_row, rows)

    for n in range(2):
        task(("norm", n), all_tokens + ["prepare"], 0.65, 2, lambda n=n: norm_tokens(n))

    def columns_of(n):
        return slice(n * 256, (n + 1) * 256)

    def project(weights, dest, b):
        at = plane_rows(b)

        @pl.loop(0, 2)
        def _(n):
            columns = pl.ds(pl.multiple_of(n * 256, 256), 256)
            value = jnp.dot(normed[:, at], weights[at, columns], preferred_element_type=F32)
            dest[:, columns] = value if b == 0 else dest[:, columns] + value

    def round_values():
        values[...] = raw_value[...].astype(BF)

    def rotary():
        @pl.loop(0, ROWS // 64)
        def _(i):
            rows = pl.ds(pl.multiple_of(i * 64, 64), 64)
            c, s = cos_tab[rows, :], sin_tab[rows, :]
            for start, dest, factor in ((0, query, 1.0), (DK, keys, DK**-0.5)):
                first, second = raw[rows, start : start + 128], raw[rows, start + 128 : start + 256]
                dest[rows, 0:128] = ((first * c - second * s) * factor).astype(BF)
                dest[rows, 128:256] = ((second * c + first * s) * factor).astype(BF)

    before = [("norm", 0), ("norm", 1)]
    for u, dest, name in ((0, raw, "both"), (1, raw_value, "value")):
        last = []
        for b in planes:
            task(
                (name, b), of_plane(u, b) + before + last, 0.6, 3,
                lambda u=u, dest=dest, b=b: project(units[u], dest, b),
            )
            last = [(name, b)]
    task("rotary", [("both", 2)], 0.25, 3, rotary)
    task("values", [("value", 2)], 0.1, 3, round_values)

    def retain(i):
        gain = head_rows[pl.ds(tp, 1), :]
        rows = slice(i * 128, (i + 1) * 128)
        total = jnp.zeros((128, DV), F32)
        for j in range(i + 1):
            there = slice(j * 128, (j + 1) * 128)
            score = turned_dot(query[rows, :], keys[there, :]) * decay[i - j]
            total = total + jnp.dot(score.astype(BF), values[there, :], preferred_element_type=F32)
        scale = lax.rsqrt(jnp.mean(total * total, axis=-1, keepdims=True) + HEAD_EPS)
        head_out[rows, :] = (total * scale * gain).astype(BF)

    for i in range(4):
        task(("retain", i), ["rotary", "values"], 0.4 + 0.1 * i, 3, lambda i=i: retain(i))

    def reduce(tag, i, needs, cost, compute, buffers, part, half, size, settle, settle_cost):
        give, take, move, left, right, through = buffers
        task((tag, "terms", i), needs, cost, 3 + i, compute)
        message(
            (tag, "give", i), (tag, "terms", i), "partner", 8 * size, give.at[i], take.at[i], take.at[i],
            None, None, ((tag, "give"), give),
        )

        def spread():
            for n, (o, h) in enumerate(((2, 0), (2, 1), (1, 1), (-1, 0))):
                move[i, n] = part(i, o, h).astype(BF)

        task((tag, "spread", i), [(tag, "give", i)], 0.1, 1, spread)
        for n, (link, dest) in enumerate(
            (
                (("x", 1), through.at[i, 0]),
                (("x", -1), through.at[i, 1]),
                (("x", 1), left.at[(i, *half(1))]),
                (("x", -1), right.at[(i, *half(0))]),
                (("x", 1), left.at[(i, *half(0))]),
                (("x", -1), right.at[(i, *half(1))]),
            )
        ):
            after = (tag, "spread", i) if n < 4 else (tag, "merge", i, n - 4)
            message((tag, "move", i, n), after, link, size, move.at[i, n], dest, dest, (*XRANK[tag, i], (1, 1, 2, 2, 0, 0)[n]),
                None if n < 2 else ((tag, "last", i), move.at[i, pl.ds(0, 4)]), ((tag, "move"), move))

        def merge(h):
            o = 1 if h == 0 else -1
            move[i, 4 + h] = (part(i, o, h) + through[i, h].astype(F32)).astype(BF)

        for h in range(2):
            task(
                (tag, "merge", i, h), [(tag, "move", i, h), (tag, "spread", i)], 0.06, 0, lambda h=h: merge(h)
            )
        needs = [(tag, "spread", i)] + [(tag, "move", i, n) for n in range(2, 6)]
        return needs, settle_cost, settle

    def half1(h):
        return (slice(h * 32, (h + 1) * 32), slice(None))

    def part1(i, o, h):
        rows, columns = half1(h)
        return terms1[i, core, at_x(o), rows, columns] + take1[i, at_x(o), rows, columns].astype(F32)

    def out_terms(i):
        at = pl.multiple_of(plane(planes[i]) * 512, 512)
        for n in range(2):
            value = turned_dot(head_out[...], w_out[pl.ds(at + n * 256, 256), :])
            terms1[i, :, :, :, columns_of(n)] = value.reshape(2, 4, 64, 256)
        give1[i] = terms1[i, 1 - core].astype(BF)

    def token_rows(o, c, h=None):
        start, size = (0, 64) if h is None else (h * 32, 32)
        return pl.ds(pl.multiple_of(c * 256 + at_x(o) * 64 + start, size), size)

    def settle1(i):
        p = plane(planes[i])
        rows = token_rows(0, core)
        total = terms1[i, core, x] + take1[i, x].astype(F32) + left1[i].astype(F32) + right1[i].astype(F32)
        for n in range(2):
            middle[p, rows, columns_of(n)] = (total[:, columns_of(n)] + blocks[2 * p + n, rows, :].astype(F32)).astype(BF)

    def middle_view(i):
        return lambda o, c, h: middle.at[plane(planes[i]), token_rows(o, c, h)]

    def norm_middle(i):
        @pl.loop(0, 2)
        def _(n):
            rows = pl.ds(pl.multiple_of(i * 128 + n * 64, 64), 64)
            scaled(normed, lambda b, r: middle[b // 2, r, columns_of(b % 2)], chan_row, rows)

    def mix_up(i):
        rows = slice(i * 128, (i + 1) * 128)
        for n in range(2):
            value = jnp.maximum(
                jnp.dot(normed[rows, :], w_up[:, columns_of(n)], preferred_element_type=F32), 0.0
            )
            hidden[rows, columns_of(n)] = (value * value).astype(BF)

    def half2(h):
        return (slice(h * 64, (h + 1) * 64), slice(None))

    def part2(i, o, h):
        rows, columns = half2(h)
        return terms2[i, at_x(o), core, rows, columns] + take2[i, at_x(o), rows, columns].astype(F32)

    def down_terms(i):
        rows = slice(i * 128, (i + 1) * 128)

        for n in range(8):
            value = jnp.dot(hidden[rows, :], down_turned[:, columns_of(n)], preferred_element_type=F32)
            terms2[i, n // 2, n % 2] = value

        for n in range(4):
            give2[i, n] = terms2[i, n, 1 - core].astype(BF)

    def settle2(i):
        rows = slice(i * 128, (i + 1) * 128)
        total = terms2[i, x, core] + take2[i, x].astype(F32)
        total = total + left2[i].astype(F32) + right2[i].astype(F32)
        columns = pl.ds(pl.multiple_of(core * 256, 256), 256)
        answer[rows, :] = (total + middle[x, rows, columns].astype(F32)).astype(BF)
        pltpu.make_async_copy(answer.at[rows], result.at[rows], local_sem.at[i]).start()

    pieces = []
    for i, b in enumerate(planes):
        needs, cost, body = reduce(
            "m", i, of_plane(2, b) + [("retain", n) for n in range(4)], 0.5, lambda i=i: out_terms(i),
            (give1, take1, move1, left1, right1, pass1), part1, half1, 32768, lambda i=i: settle1(i), 0.08,
        )
        pieces += gather(
            ("c", i), middle_view(i), 32768, (cost, body), needs, XRANK["c", i],
            middle.at[0, pl.ds(0, 256)], ("c", middle.at[:, pl.ds(0, 448)]),
        )
    for i in range(4):
        task(("norm2", i), pieces + [("both", 2), ("value", 2)], 0.32, 3 + i, lambda i=i: norm_middle(i))
        task(("up", i), inside[3] + [("norm2", i)], 0.45, 3 + i, lambda i=i: mix_up(i))
        needs, cost, body = reduce(
            "d", i, turned + [("up", i)], 0.52, lambda i=i: down_terms(i),
            (give2, take2, move2, left2, right2, pass2), part2, half2, 32768, lambda i=i: settle2(i), 0.08,
        )
        task(("last", i), needs, cost, 1, body)

    items, _ = schedule(tasks, messages)
    number = {n: k for k, n in enumerate(dict.fromkeys(lands.values()))}
    sender = {n: k for k, n in enumerate(totals)}
    assert len(number) <= LANDS and len(sender) <= SENDS, "semaphores"

    def start(name):
        source, dest, _ = views[name]
        copy = pltpu.make_async_remote_copy(
            src_ref=source,
            dst_ref=dest,
            send_sem=send_sem.at[sender[leaves[name]]],
            recv_sem=recv_sem.at[number[lands[name]]],
            device_id=target[messages[name][1]],
            device_id_type=MESH,
        )
        copy.start()

    departing = defaultdict(list)
    for name, (after, _, _, rank) in messages.items():
        if rank is None:
            departing[after].append(name)
    for _, _, _, kind, name in items:
        if kind == "send":
            start(name)
            continue
        waits = [n for n in tasks[name][0] if n in messages]
        if waits:
            for key in dict.fromkeys(lands[n] for n in waits):
                here = next(views[n][2] for n in waits if lands[n] == key)
                pltpu.make_async_copy(here, here, recv_sem.at[number[key]]).wait()
        if bodies[name]:
            bodies[name]()
        for n in departing[name]:
            start(n)
    for i in range(4):
        rows = slice(i * 128, (i + 1) * 128)
        pltpu.make_async_copy(answer.at[rows], result.at[rows], local_sem.at[i]).wait()
    for key, whole in totals.items():
        pltpu.make_async_copy(whole, whole, send_sem.at[sender[key]]).wait()


def rotary_tables():
    half = DK // 2
    angle = np.arange(ROWS)[:, None] * THETA ** (-np.arange(half) / half)
    return np.cos(angle).astype(np.float32), np.sin(angle).astype(np.float32)


def shards(tokens, mix_gain, query_w, key_w, value_w, head_gain, out_w, chan_gain, up_w, down_w):
    cosine, sine = rotary_tables()
    any_place = pl.BlockSpec(memory_space=pl.ANY)
    vmem = pltpu.VMEM
    scratch = [
        *[vmem((D, 512), BF)] * 5,
        vmem((512, D), BF),
        vmem((8, ROWS, 256), BF),
        vmem((ROWS, D), BF),
        vmem((4, ROWS, 512), BF),
        vmem((1, D), F32),
        vmem((1, D), F32),
        vmem((8, DV), F32),
        vmem((ROWS, DK // 2), F32),
        vmem((ROWS, DK // 2), F32),
        vmem((4, 128, 128), F32),
        vmem((ROWS, 512), F32),
        vmem((ROWS, 512), F32),
        vmem((ROWS, DK), BF),
        vmem((ROWS, DK), BF),
        vmem((ROWS, DV), BF),
        vmem((ROWS, DV), BF),
        vmem((ROWS, 512), BF),
        vmem((4, 2, 4, 64, 512), F32),
        vmem((4, 4, 64, 512), BF),
        vmem((4, 4, 64, 512), BF),
        vmem((4, 6, 32, 512), BF),
        vmem((4, 64, 512), BF),
        vmem((4, 64, 512), BF),
        vmem((4, 2, 32, 512), BF),
        vmem((4, 4, 2, 128, 256), F32),
        vmem((4, 4, 128, 256), BF),
        vmem((4, 4, 128, 256), BF),
        vmem((4, 6, 64, 256), BF),
        vmem((4, 128, 256), BF),
        vmem((4, 128, 256), BF),
        vmem((4, 2, 64, 256), BF),
        vmem((ROWS, 256), BF),
        pltpu.SemaphoreType.DMA((12,)),
        pltpu.SemaphoreType.DMA((SENDS,)),
        pltpu.SemaphoreType.DMA((LANDS,)),
    ]
    whole = pl.pallas_call(
        layer_kernel,
        out_shape=jax.ShapeDtypeStruct((ROWS, 256), BF),
        in_specs=[any_place] * 12,
        out_specs=any_place,
        scratch_shapes=scratch,
        compiler_params=pltpu.CompilerParams(
            collective_id=0, has_side_effects=True, vmem_limit_bytes=60 << 20
        ),
        name="layer",
    )(
        tokens, mix_gain.reshape(1, D), query_w, key_w, value_w, head_gain, out_w.T,
        chan_gain.reshape(1, D), up_w, down_w.T, jnp.asarray(cosine), jnp.asarray(sine),
    )
    return whole


def solution(mesh):
    placed = (
        P(("rep", "fs"), "tp"),
        P(),
        P("fs", "tp"),
        P("fs", "tp"),
        P("fs", "tp"),
        P(),
        P("tp", "fs"),
        P(),
        P("fs", "tp"),
        P("tp", "fs"),
    )
    return jax.shard_map(
        shards, mesh=mesh, in_specs=placed, out_specs=P(("rep", "fs"), "tp"), check_vma=False
    )
```

```python
import heapq
from collections import defaultdict

import jax
import jax.numpy as jnp
import numpy as np
from jax import lax
from jax.experimental import pallas as pl
from jax.experimental.pallas import tpu as pltpu
from jax.sharding import PartitionSpec as P

ROWS = 512
D = 2048
DK = 256
DV = 512
EPS = 1e-06
HEAD_EPS = 0.05
THETA = 10000.0
NX, NY, NZ = 4, 8, 4
MESH = pl.DeviceIdType.MESH
BF, F32 = jnp.bfloat16, jnp.float32

PARTS = (
    (0, 0, 64, "A", 0, 0.0),
    (1, 0, 64, "B", 1, 0.0),
    (2, 0, 64, "A", 1, 1.5),
    (3, 0, 64, "B", 2, 2.5),
    (4, 0, 64, "A", 2, 2.5),
)
SENDS, LANDS = 11, 175
LEAD = {"y": 1.5, "z": 1.5, "x": 1.2}
XRANK = {(t, i): (i + 1.5 * k, k) for k, t in enumerate("mcd") for i in range(4)}
RATE = {"ring": 45.2e3, "partner": 600e3}
DELAY = {"early": 2.3, "late": 2.5, "x": 2.2, "partner": 1.1}


def onward(p, a, b):
    out = []
    two = lambda k: 1 if k % 2 == 0 else -1
    if PARTS[p][3] == "A":
        fw = 4 if p % 4 < 2 else 3
        if b == 0:
            if 0 <= a < fw:
                out.append(("y", 1))
            if 0 >= a > fw - 7:
                out.append(("y", -1))
            out += [("z", 1), ("z", -1)]
        elif abs(b) == 1 and two(a) == b:
            out.append(("z", b))
    else:
        fw = 4 if b % 2 == 0 else 3
        if a == 0:
            if b == 0:
                out += [("z", 1), ("z", -1)]
            elif abs(b) == 1 and two(p // 2) == b:
                out.append(("z", b))
        if 0 <= a < fw:
            out.append(("y", 1))
        if 0 >= a > fw - 7:
            out.append(("y", -1))
    return [(k, a + k[1] * (k[0] == "y"), b + k[1] * (k[0] == "z")) for k in out]


def below(p, a, b):
    return max([0] + [1 + below(p, na, nb) for _, na, nb in onward(p, a, b)])


def schedule(tasks, messages):
    left, users, leaving = {}, defaultdict(list), defaultdict(list)
    for name, (needs, _, _, start) in tasks.items():
        left[name] = len(needs) + 1
        for need in needs:
            users[need].append(name)
    for name, (task, *_) in messages.items():
        leaving[task].append(name)
    events, ready, items = [], [], []
    count = 0
    link_free = defaultdict(float)
    queue = defaultdict(list)
    core_free = 0.0
    for name, (_, _, _, start) in tasks.items():
        heapq.heappush(events, (start, count, "part", name))
        count += 1
    now = 0.0

    def serve(link, time):
        nonlocal count
        while queue[link] and link_free[link] <= time + 1e-9:
            message = heapq.heappop(queue[link])[-1]
            kind = "partner" if link == "partner" else "ring"
            begin = max(time, link_free[link])
            link_free[link] = begin + messages[message][2] / RATE[kind]
            if messages[message][3] is not None:
                items.append((max(available[message], begin - LEAD[link[0]]), 1, len(items), "send", message))
            rank = messages[message][3]
            delay = DELAY["partner" if link == "partner" else "x" if link[0] == "x" else "early" if rank[0] < 2 else "late"]
            heapq.heappush(events, (link_free[link] + delay, count, "arrive", message))
            heapq.heappush(events, (link_free[link], count + 1, "link", link))
            count += 2

    available, arrived, done = {}, {}, {}
    while events:
        now, _, kind, name = heapq.heappop(events)
        if kind == "link":
            serve(name, now)
        elif kind == "free":
            done[name] = now
            for message in leaving[name]:
                task, link, size, rank = messages[message]
                available[message] = now
                heapq.heappush(queue[link], ((99, now) if rank is None else rank, count, message))
                count += 1
                serve(link, now)
        targets = [name] if kind == "part" else users[name] if kind in ("arrive", "free") else []
        if kind == "arrive":
            arrived[name] = now
        for task in targets:
            left[task] -= 1
            if left[task] == 0:
                heapq.heappush(ready, (tasks[task][2], count, task))
                count += 1
        while ready and core_free <= now + 1e-9:
            if events and events[0][0] <= now + 1e-9 and events[0][2] != "link":
                break
            task = heapq.heappop(ready)[-1]
            items.append((now, 0, len(items), "task", task))
            core_free = now + tasks[task][1]
            heapq.heappush(events, (core_free, count, "free", task))
            count += 1
    assert len(done) == len(tasks), "cycle"
    items.sort()
    sent = set()
    for _, _, _, kind, name in items:
        if kind == "send":
            sent.add(name)
        else:
            assert all(n in done or n in sent for n in tasks[name][0]), "order"
            sent.update(m for m in leaving[name] if messages[m][3] is None)
    return items, done


def turned_dot(left, right):
    return lax.dot_general(left, right, (((1,), (1,)), ((), ())), preferred_element_type=F32)


def layer_kernel(
    tokens, mix_gain, query_w, key_w, value_w, head_gain, out_w, chan_gain, up_w, down_w, cosine, sine,
    result,
    w_both, w_value, w_out, w_up, w_down, down_turned,
    blocks, normed, middle, mix_row, chan_row, head_rows, cos_tab, sin_tab, decay,
    raw, raw_value, query, keys, values, head_out, hidden,
    terms1, give1, take1, move1, left1, right1, pass1,
    terms2, give2, take2, move2, left2, right2, pass2,
    answer, local_sem, send_sem, recv_sem,
):
    rep, fs, tp = lax.axis_index("rep"), lax.axis_index("fs"), lax.axis_index("tp")
    z, y = fs // NY, fs % NY
    x, core = tp // 2, tp % 2
    units = (w_both, w_value, w_out, w_up, w_down)
    target = {
        ("y", 1): {"fs": z * NY + (y + 1) % NY},
        ("y", -1): {"fs": z * NY + (y + NY - 1) % NY},
        ("z", 1): {"rep": (rep + (z + 1) // NZ) % 2, "fs": ((z + 1) % NZ) * NY + y},
        ("z", -1): {"rep": (rep + (NZ - z) // NZ) % 2, "fs": ((z + NZ - 1) % NZ) * NY + y},
        ("x", 1): {"tp": ((x + 1) % NX) * 2 + core},
        ("x", -1): {"tp": ((x + NX - 1) % NX) * 2 + core},
        "partner": {"tp": x * 2 + (1 - core)},
    }
    barrier = pltpu.get_barrier_semaphore()
    for k in target:
        pl.semaphore_signal(barrier, inc=1, device_id=target[k], device_id_type=MESH)

    def slot(a, b):
        at = ((z - b + NZ) % NZ) * NY + (y - a + NY) % NY
        return pl.ds(pl.multiple_of(at * 64, 64), 64)

    mine = slot(0, 0)
    local = []

    def bring(source, dest):
        copy = pltpu.make_async_copy(source, dest, local_sem.at[len(local)])
        copy.start()
        local.append(copy)

    bring(tokens, blocks.at[tp])
    bring(query_w, w_both.at[mine, 0:DK])
    bring(key_w, w_both.at[mine, DK : 2 * DK])
    bring(value_w, w_value.at[mine])
    bring(out_w, w_out.at[mine])
    bring(up_w, w_up.at[mine])
    bring(down_w, w_down.at[mine])
    bring(mix_gain, mix_row)
    bring(chan_gain, chan_row)
    bring(head_gain, head_rows)
    bring(cosine, cos_tab)
    bring(sine, sin_tab)
    for copy in local[:4]:
        copy.wait()
    pl.semaphore_wait(barrier, len(target))

    tasks, bodies = {}, {}
    messages, views = {}, {}
    lands, leaves, totals = {}, {}, {}

    def task(name, needs, cost, rank, body=None, start=0.0):
        tasks[name] = (needs, cost, rank, start)
        bodies[name] = body

    def message(name, after, link, size, source, dest, here, rank=None, share=None, sent=None):
        messages[name] = (after, link, size, rank)
        views[name] = (source, dest, share[1] if share else here)
        lands[name] = share[0] if share else name
        leaves[name] = sent[0]
        totals[sent[0]] = sent[1]

    def piece(p, a, b):
        u, first, count = PARTS[p][:3]
        at = ((z - b + NZ) % NZ) * NY + (y - a + NY) % NY
        return units[u].at[pl.ds(pl.multiple_of(at * 64 + first, 16), count)]

    inside = defaultdict(list)
    for p, (u, _, count, _, rank, start) in enumerate(PARTS):
        stack, ends = [(0, 0)], defaultdict(list)
        sent = (("w", p), units[u].at[pl.ds(0, 31 * count)])
        seen = {}
        while stack:
            a, b = stack.pop()
            seen[a, b] = onward(p, a, b)
            if not seen[a, b]:
                ends[2 if abs(b) == 2 else b].append((a, b))
            stack += [(na, nb) for _, na, nb in seen[a, b]]
        for (a, b), following in seen.items():
            if not following:
                continue
            name = ("w", p, a, b)
            needs = ([] if u < 2 else ["prepare"]) if (a, b) == (0, 0) else [name]
            task(("got", *name), needs, 0.02, -1, None, start)
            inside[u].append(("got", *name))
            for k, na, nb in following:
                group = [(g, e) for g, e in ends.items() if (na, nb) in e]
                share = None
                if group:
                    share = (("end", p, group[0][0]), units[u].at[pl.ds(0, len(group[0][1]) * count)])
                message(
                    ("w", p, na, nb), ("got", *name), k, count * 1024,
                    piece(p, a, b), piece(p, a, b), piece(p, na, nb), (rank, -1 - below(p, na, nb)), share, sent,
                )
        for g, group in ends.items():
            name = ("got", "w", p, "end", g)
            task(name, [("w", p, a, b) for a, b in group], 0.02, 1, None)
            inside[u].append(name)

    planes = (0, 1, -1, 2)

    def plane(b):
        return (z - b + NZ) % NZ

    def of_plane(u, b):
        return [n for n in inside[u] if n[-1] in ((2, -2) if b == 2 else (b,))]

    def plane_rows(b):
        return pl.ds(pl.multiple_of(plane(b) * 512, 512), 512)

    def turn(b):
        at = pl.multiple_of(plane(b) * 512, 512)
        for n in range(4):
            down_turned[:, pl.ds(at + n * 128, 128)] = w_down[pl.ds(at + n * 128, 128), :].T

    for b in planes:
        task(("turn", b), of_plane(4, b), 0.22, 2, lambda b=b: turn(b))
    turned = [("turn", b) for b in planes]

    def at_x(o):
        return (x + o + NX) % NX

    def gather(tag, view, size, first, needs, rank, ref, sent):
        task((tag, 0, 0), needs, 0.01 if first is None else first[0], 0, first and first[1])
        parts = [(0, 0), (-1, 0), (1, 1), (-1, 1), (1, 0), (-2, 0), (2, 1)]
        for o, h in parts[1:]:
            task((tag, o, h), [(tag, "m", o, h)], 0.02, 0)
        task((tag, "p"), [(tag, "mp", o, h) for o, h in parts + [(0, 1)]], 0.02, 1)

        def pass_on(o, h, after, link, no):
            message((tag, "m", no, h), after, link, size, view(o, core, h), view(o, core, h), view(no, core, h), (*rank, 0 if no in (-2, 2) else 1), None, sent)

        pass_on(0, 0, (tag, 0, 0), ("x", 1), -1)
        pass_on(0, 1, (tag, 0, 0), ("x", -1), 1)
        pass_on(0, 1, (tag, 0, 0), ("x", 1), -1)
        pass_on(0, 0, (tag, 0, 0), ("x", -1), 1)
        pass_on(-1, 0, (tag, -1, 0), ("x", 1), -2)
        pass_on(1, 1, (tag, 1, 1), ("x", -1), 2)
        for o, h in parts + [(0, 1)]:
            after = (tag, 0, 0) if o == 0 else (tag, o, h)
            message(
                (tag, "mp", o, h), after, "partner", size,
                view(o, core, h), view(o, core, h), view(o, 1 - core, h), None, ((tag, "p"), ref), sent,
            )
        return [(tag, o, h) for o, h in parts] + [(tag, "p")]

    def token_view(o, c, h):
        return blocks.at[at_x(o) * 2 + c, pl.ds(h * 256, 256)]

    all_tokens = gather("t", token_view, 131072, None, [], (0, 0), blocks.at[pl.ds(0, 4)], ("t", blocks.at[pl.ds(0, 7)]))

    def prepare():
        for copy in local[4:]:
            copy.wait()
        rate = jnp.float32(0.0)
        for h in range(8):
            rate = jnp.where(tp == h, jnp.float32(np.log1p(-(2.0 ** (-5 - h)))), rate)
        offset = (
            lax.broadcasted_iota(jnp.int32, (128, 128), 0) - lax.broadcasted_iota(jnp.int32, (128, 128), 1)
        ).astype(F32)
        for n in range(4):
            value = jnp.exp(rate * jnp.maximum(offset + 128.0 * n, 0.0))
            decay[n] = jnp.where(offset + 128.0 * n >= 0, value, 0.0)

    task("prepare", [], 0.4, -2, prepare, 0.5)

    def scaled(dest, read, gain, rows):
        total = jnp.zeros((64, 256), F32)
        for b in range(8):
            part = read(b, rows).astype(F32)
            total = total + part * part
        scale = lax.rsqrt(jnp.sum(total, axis=-1, keepdims=True) * (1.0 / D) + EPS)
        for b in range(8):
            columns = slice(b * 256, (b + 1) * 256)
            dest[rows, columns] = (read(b, rows).astype(F32) * scale * gain[:, columns]).astype(BF)

    def norm_tokens(n):
        @pl.loop(0, 4)
        def _(i):
            rows = pl.ds(pl.multiple_of(n * 256 + i * 64, 64), 64)
            scaled(normed, lambda b, r: blocks[b, r, :], mix_row, rows)

    for n in range(2):
        task(("norm", n), all_tokens + ["prepare"], 0.65, 2, lambda n=n: norm_tokens(n))

    def columns_of(n):
        return slice(n * 256, (n + 1) * 256)

    def project(weights, dest, b):
        at = plane_rows(b)

        @pl.loop(0, 2)
        def _(n):
            columns = pl.ds(pl.multiple_of(n * 256, 256), 256)
            value = jnp.dot(normed[:, at], weights[at, columns], preferred_element_type=F32)
            dest[:, columns] = value if b == 0 else dest[:, columns] + value

    def round_values():
        values[...] = raw_value[...].astype(BF)

    def rotary():
        @pl.loop(0, ROWS // 64)
        def _(i):
            rows = pl.ds(pl.multiple_of(i * 64, 64), 64)
            c, s = cos_tab[rows, :], sin_tab[rows, :]
            for start, dest, factor in ((0, query, 1.0), (DK, keys, DK**-0.5)):
                first, second = raw[rows, start : start + 128], raw[rows, start + 128 : start + 256]
                dest[rows, 0:128] = ((first * c - second * s) * factor).astype(BF)
                dest[rows, 128:256] = ((second * c + first * s) * factor).astype(BF)

    before = [("norm", 0), ("norm", 1)]
    for u, dest, name in ((0, raw, "both"), (1, raw_value, "value")):
        last = []
        for b in planes:
            task(
                (name, b), of_plane(u, b) + before + last, 0.6, 3,
                lambda u=u, dest=dest, b=b: project(units[u], dest, b),
            )
            last = [(name, b)]
    task("rotary", [("both", 2)], 0.25, 3, rotary)
    task("values", [("value", 2)], 0.1, 3, round_values)

    def retain(i):
        gain = head_rows[pl.ds(tp, 1), :]
        rows = slice(i * 128, (i + 1) * 128)
        total = jnp.zeros((128, DV), F32)
        for j in range(i + 1):
            there = slice(j * 128, (j + 1) * 128)
            score = turned_dot(query[rows, :], keys[there, :]) * decay[i - j]
            total = total + jnp.dot(score.astype(BF), values[there, :], preferred_element_type=F32)
        scale = lax.rsqrt(jnp.mean(total * total, axis=-1, keepdims=True) + HEAD_EPS)
        head_out[rows, :] = (total * scale * gain).astype(BF)

    for i in range(4):
        task(("retain", i), ["rotary", "values"], 0.4 + 0.1 * i, 3, lambda i=i: retain(i))

    def reduce(tag, i, needs, cost, compute, buffers, part, half, size, settle, settle_cost):
        give, take, move, left, right, through = buffers
        task((tag, "terms", i), needs, cost, 3 + i, compute)
        message(
            (tag, "give", i), (tag, "terms", i), "partner", 8 * size, give.at[i], take.at[i], take.at[i],
            None, None, ((tag, "give"), give),
        )

        def spread():
            for n, (o, h) in enumerate(((2, 0), (2, 1), (1, 1), (-1, 0))):
                move[i, n] = part(i, o, h).astype(BF)

        task((tag, "spread", i), [(tag, "give", i)], 0.1, 1, spread)
        for n, (link, dest) in enumerate(
            (
                (("x", 1), through.at[i, 0]),
                (("x", -1), through.at[i, 1]),
                (("x", 1), left.at[(i, *half(1))]),
                (("x", -1), right.at[(i, *half(0))]),
                (("x", 1), left.at[(i, *half(0))]),
                (("x", -1), right.at[(i, *half(1))]),
            )
        ):
            after = (tag, "spread", i) if n < 4 else (tag, "merge", i, n - 4)
            message((tag, "move", i, n), after, link, size, move.at[i, n], dest, dest, (*XRANK[tag, i], (1, 1, 2, 2, 0, 0)[n]),
                None if n < 2 else ((tag, "last", i), move.at[i, pl.ds(0, 4)]), ((tag, "move"), move))

        def merge(h):
            o = 1 if h == 0 else -1
            move[i, 4 + h] = (part(i, o, h) + through[i, h].astype(F32)).astype(BF)

        for h in range(2):
            task(
                (tag, "merge", i, h), [(tag, "move", i, h), (tag, "spread", i)], 0.06, 0, lambda h=h: merge(h)
            )
        needs = [(tag, "spread", i)] + [(tag, "move", i, n) for n in range(2, 6)]
        return needs, settle_cost, settle

    def half1(h):
        return (slice(h * 32, (h + 1) * 32), slice(None))

    def part1(i, o, h):
        rows, columns = half1(h)
        return terms1[i, core, at_x(o), rows, columns] + take1[i, at_x(o), rows, columns].astype(F32)

    def out_terms(i):
        at = pl.multiple_of(plane(planes[i]) * 512, 512)
        for n in range(2):
            value = turned_dot(head_out[...], w_out[pl.ds(at + n * 256, 256), :])
            terms1[i, :, :, :, columns_of(n)] = value.reshape(2, 4, 64, 256)
        give1[i] = terms1[i, 1 - core].astype(BF)

    def token_rows(o, c, h=None):
        start, size = (0, 64) if h is None else (h * 32, 32)
        return pl.ds(pl.multiple_of(c * 256 + at_x(o) * 64 + start, size), size)

    def settle1(i):
        p = plane(planes[i])
        rows = token_rows(0, core)
        total = terms1[i, core, x] + take1[i, x].astype(F32) + left1[i].astype(F32) + right1[i].astype(F32)
        for n in range(2):
            middle[p, rows, columns_of(n)] = (total[:, columns_of(n)] + blocks[2 * p + n, rows, :].astype(F32)).astype(BF)

    def middle_view(i):
        return lambda o, c, h: middle.at[plane(planes[i]), token_rows(o, c, h)]

    def norm_middle(i):
        @pl.loop(0, 2)
        def _(n):
            rows = pl.ds(pl.multiple_of(i * 128 + n * 64, 64), 64)
            scaled(normed, lambda b, r: middle[b // 2, r, columns_of(b % 2)], chan_row, rows)

    def mix_up(i):
        rows = slice(i * 128, (i + 1) * 128)
        for n in range(2):
            value = jnp.maximum(
                jnp.dot(normed[rows, :], w_up[:, columns_of(n)], preferred_element_type=F32), 0.0
            )
            hidden[rows, columns_of(n)] = (value * value).astype(BF)

    def half2(h):
        return (slice(h * 64, (h + 1) * 64), slice(None))

    def part2(i, o, h):
        rows, columns = half2(h)
        return terms2[i, at_x(o), core, rows, columns] + take2[i, at_x(o), rows, columns].astype(F32)

    def down_terms(i):
        rows = slice(i * 128, (i + 1) * 128)

        for n in range(8):
            value = jnp.dot(hidden[rows, :], down_turned[:, columns_of(n)], preferred_element_type=F32)
            terms2[i, n // 2, n % 2] = value

        for n in range(4):
            give2[i, n] = terms2[i, n, 1 - core].astype(BF)

    def settle2(i):
        rows = slice(i * 128, (i + 1) * 128)
        total = terms2[i, x, core] + take2[i, x].astype(F32)
        total = total + left2[i].astype(F32) + right2[i].astype(F32)
        columns = pl.ds(pl.multiple_of(core * 256, 256), 256)
        answer[rows, :] = (total + middle[x, rows, columns].astype(F32)).astype(BF)
        pltpu.make_async_copy(answer.at[rows], result.at[rows], local_sem.at[i]).start()

    pieces = []
    for i, b in enumerate(planes):
        needs, cost, body = reduce(
            "m", i, of_plane(2, b) + [("retain", n) for n in range(4)], 0.5, lambda i=i: out_terms(i),
            (give1, take1, move1, left1, right1, pass1), part1, half1, 32768, lambda i=i: settle1(i), 0.08,
        )
        pieces += gather(
            ("c", i), middle_view(i), 32768, (cost, body), needs, XRANK["c", i],
            middle.at[0, pl.ds(0, 256)], ("c", middle.at[:, pl.ds(0, 448)]),
        )
    for i in range(4):
        task(("norm2", i), pieces + [("both", 2), ("value", 2)], 0.32, 3 + i, lambda i=i: norm_middle(i))
        task(("up", i), inside[3] + [("norm2", i)], 0.45, 3 + i, lambda i=i: mix_up(i))
        needs, cost, body = reduce(
            "d", i, turned + [("up", i)], 0.52, lambda i=i: down_terms(i),
            (give2, take2, move2, left2, right2, pass2), part2, half2, 32768, lambda i=i: settle2(i), 0.08,
        )
        task(("last", i), needs, cost, 1, body)

    items, _ = schedule(tasks, messages)
    number = {n: k for k, n in enumerate(dict.fromkeys(lands.values()))}
    sender = {n: k for k, n in enumerate(totals)}
    assert len(number) <= LANDS and len(sender) <= SENDS, "semaphores"

    def start(name):
        source, dest, _ = views[name]
        copy = pltpu.make_async_remote_copy(
            src_ref=source,
            dst_ref=dest,
            send_sem=send_sem.at[sender[leaves[name]]],
            recv_sem=recv_sem.at[number[lands[name]]],
            device_id=target[messages[name][1]],
            device_id_type=MESH,
        )
        copy.start()

    departing = defaultdict(list)
    for name, (after, _, _, rank) in messages.items():
        if rank is None:
            departing[after].append(name)
    for _, _, _, kind, name in items:
        if kind == "send":
            start(name)
            continue
        waits = [n for n in tasks[name][0] if n in messages]
        if waits:
            for key in dict.fromkeys(lands[n] for n in waits):
                here = next(views[n][2] for n in waits if lands[n] == key)
                pltpu.make_async_copy(here, here, recv_sem.at[number[key]]).wait()
        if bodies[name]:
            bodies[name]()
        for n in departing[name]:
            start(n)
    for i in range(4):
        rows = slice(i * 128, (i + 1) * 128)
        pltpu.make_async_copy(answer.at[rows], result.at[rows], local_sem.at[i]).wait()
    for key, whole in totals.items():
        pltpu.make_async_copy(whole, whole, send_sem.at[sender[key]]).wait()


def rotary_tables():
    half = DK // 2
    angle = np.arange(ROWS)[:, None] * THETA ** (-np.arange(half) / half)
    return np.cos(angle).astype(np.float32), np.sin(angle).astype(np.float32)


def shards(tokens, mix_gain, query_w, key_w, value_w, head_gain, out_w, chan_gain, up_w, down_w):
    cosine, sine = rotary_tables()
    any_place = pl.BlockSpec(memory_space=pl.ANY)
    vmem = pltpu.VMEM
    scratch = [
        *[vmem((D, 512), BF)] * 5,
        vmem((512, D), BF),
        vmem((8, ROWS, 256), BF),
        vmem((ROWS, D), BF),
        vmem((4, ROWS, 512), BF),
        vmem((1, D), F32),
        vmem((1, D), F32),
        vmem((8, DV), F32),
        vmem((ROWS, DK // 2), F32),
        vmem((ROWS, DK // 2), F32),
        vmem((4, 128, 128), F32),
        vmem((ROWS, 512), F32),
        vmem((ROWS, 512), F32),
        vmem((ROWS, DK), BF),
        vmem((ROWS, DK), BF),
        vmem((ROWS, DV), BF),
        vmem((ROWS, DV), BF),
        vmem((ROWS, 512), BF),
        vmem((4, 2, 4, 64, 512), F32),
        vmem((4, 4, 64, 512), BF),
        vmem((4, 4, 64, 512), BF),
        vmem((4, 6, 32, 512), BF),
        vmem((4, 64, 512), BF),
        vmem((4, 64, 512), BF),
        vmem((4, 2, 32, 512), BF),
        vmem((4, 4, 2, 128, 256), F32),
        vmem((4, 4, 128, 256), BF),
        vmem((4, 4, 128, 256), BF),
        vmem((4, 6, 64, 256), BF),
        vmem((4, 128, 256), BF),
        vmem((4, 128, 256), BF),
        vmem((4, 2, 64, 256), BF),
        vmem((ROWS, 256), BF),
        pltpu.SemaphoreType.DMA((12,)),
        pltpu.SemaphoreType.DMA((SENDS,)),
        pltpu.SemaphoreType.DMA((LANDS,)),
    ]
    whole = pl.pallas_call(
        layer_kernel,
        out_shape=jax.ShapeDtypeStruct((ROWS, 256), BF),
        in_specs=[any_place] * 12,
        out_specs=any_place,
        scratch_shapes=scratch,
        compiler_params=pltpu.CompilerParams(
            collective_id=0, has_side_effects=True, vmem_limit_bytes=60 << 20
        ),
        name="layer",
    )(
        tokens, mix_gain.reshape(1, D), query_w, key_w, value_w, head_gain, out_w.T,
        chan_gain.reshape(1, D), up_w, down_w.T, jnp.asarray(cosine), jnp.asarray(sine),
    )
    return whole


def solution(mesh):
    placed = (
        P(("rep", "fs"), "tp"),
        P(),
        P("fs", "tp"),
        P("fs", "tp"),
        P("fs", "tp"),
        P(),
        P("tp", "fs"),
        P(),
        P("fs", "tp"),
        P("tp", "fs"),
    )
    return jax.shard_map(
        shards, mesh=mesh, in_specs=placed, out_specs=P(("rep", "fs"), "tp"), check_vma=False
    )
```
